512 devices in a mesh: rep: 2 (over z_hi), fs: 32 (over z_lo, y), tp: 8 (over x, core).
Axes of the slice: x: 4, y: 8, z: 8 (z_hi: 2, z_lo: 4; z = z_hi * 4 + z_lo), core: 2. Of those that a mesh axis runs over, the one named last changes fastest.
Arguments:
- late_rows: bfloat16 [16384, 2048], P(('rep', 'fs')), parts along dimension 0, may hold values from -6 to 6
- early_rows: bfloat16 [16384, 2048], P(('rep', 'fs')), parts along dimension 0, may hold values from -6 to 6
- hidden_cot: bfloat16 [16384, 5632], P(('rep', 'fs'), 'tp'), parts along dimension 0, may hold values from -6 to 6
- gate_weight: bfloat16 [2048, 5632], P('fs', 'tp'), may hold values from -0.125 to 0.125
- up_weight: bfloat16 [2048, 5632], P('fs', 'tp'), may hold values from -0.125 to 0.125
- gate_taps: bfloat16 [3, 5632], P(None, 'tp'), may hold values from -3.5 to 3.5
- up_taps: bfloat16 [3, 5632], P(None, 'tp'), may hold values from -3.5 to 3.5
- gate_grad_sum: float32 [4096, 5632], P(('rep', 'fs'), 'tp'), parts along dimension 0, may hold values from -6 to 6
- up_grad_sum: float32 [4096, 5632], P(('rep', 'fs'), 'tp'), parts along dimension 0, may hold values from -6 to 6
- gate_taps_sum: float32 [6, 5632], P('rep', 'tp'), parts along dimension 0, may hold values from -6 to 6
- up_taps_sum: float32 [6, 5632], P('rep', 'tp'), parts along dimension 0, may hold values from -6 to 6
Outputs:
- late_hidden: bfloat16 [16384, 5632], P(('rep', 'fs'), 'tp'), parts along dimension 0
- early_grad: bfloat16 [16384, 2048], P(('rep', 'fs')), parts along dimension 0
- gate_grad_next: float32 [4096, 5632], P(('rep', 'fs'), 'tp'), parts along dimension 0
- up_grad_next: float32 [4096, 5632], P(('rep', 'fs'), 'tp'), parts along dimension 0
- gate_taps_next: float32 [6, 5632], P('rep', 'tp'), parts along dimension 0
- up_taps_next: float32 [6, 5632], P('rep', 'tp'), parts along dimension 0
The draws below stay inside these ranges and needn't reach their ends.
There are 2 independent parts, one for each index of `rep`. The reference program is written for one: setup_inputs(seed, part) draws one part's arguments, and reference() takes and returns one part's arrays. A program takes and returns all parts, laid end to end along the dimension named above; an argument that names none is the same for every part. Nothing has to cross between parts.
All inputs are finite; a program needn't handle non-finite values.
Results may differ from the reference program's by a relative error of at most 0.02.
Values may be sent and summed in bfloat16 or wider, within the bound.
A program may use at most 64 MiB of HBM per device.

```python
import jax
import jax.numpy as jnp
from jax import lax

D = 2048
FF = 5632
TAPS = 3
TOK_DEV = 256
TOKENS = 8192
N_FS = 32


def strengthened(entries, stream_key, source, target, shards_of, factor):
    owner, partner = [(jnp.arange(entries.shape[position]) // (entries.shape[position] // shards_of)).reshape([-1 if axis == position else 1 for axis in range(entries.ndim)]) for position in (source, target)]
    chosen = jax.random.permutation(stream_key, shards_of)[partner]
    strong = (owner == chosen) | (owner == (partner + shards_of // 2) % shards_of)
    return jnp.where(strong, factor * entries, entries)


def levels(own_key, dims, pieces, least, high):
    def one(axis_at, parts):
        steps = jax.random.uniform(jax.random.fold_in(jax.random.fold_in(own_key, 6), axis_at), (parts,), jnp.float32, least / len(pieces), high / len(pieces))
        return jnp.repeat(jnp.exp(steps), dims[axis_at] // parts).reshape((-1,) + (1,) * (len(dims) - axis_at - 1))

    level = one(*pieces[0])
    for cut in pieces[1:]:
        level = level * one(*cut)
    return level


def bell_draw(own_key, shape, spread, bound, cuts=(), dtype=jnp.bfloat16):
    gain = levels(own_key, shape, cuts, -0.22, 0.18) if cuts else 1.0
    drawn = jax.random.normal(own_key, shape, jnp.float32) * spread * gain
    return jnp.minimum(jnp.maximum(drawn, -bound), bound).astype(dtype)


def bell_draw_with(rng, extent, width, bound, pieces, heavy, held_as=jnp.bfloat16):
    drawn = width * jax.random.normal(rng, extent, jnp.float32)
    if pieces:
        drawn = drawn * levels(rng, extent, pieces, -0.22, 0.18)
    return jnp.clip(strengthened(drawn, jax.random.fold_in(rng, 3), *heavy), -bound, bound).astype(held_as)


def setup_inputs(seed: int = 0, part: int = 0) -> dict:
    key_list = jax.random.split(jax.random.key(seed), 12)
    own_keys = jax.random.split(jax.random.fold_in(key_list[11], part), 12)
    return {
        "late_rows": bell_draw(own_keys[0], (TOKENS, D), 1.0, 6.0, ((0, 32),)),
        "early_rows": bell_draw_with(own_keys[1], (TOKENS, D), 1.0, 6.0, ((0, 32),), (0, 1, 32, 2.75)),
        "hidden_cot": bell_draw_with(own_keys[2], (TOKENS, FF), 1.0, 6.0, ((0, 32), (1, 8)), (0, 1, 32, 2.75)),
        "gate_weight": bell_draw(key_list[3], (D, FF), D ** -0.5, 0.125, ((0, 32), (1, 8))),
        "up_weight": bell_draw(key_list[4], (D, FF), D ** -0.5, 0.125, ((0, 32), (1, 8))),
        "gate_taps": bell_draw(key_list[5], (TAPS, FF), TAPS ** -0.5, 3.5, ((1, 8),)),
        "up_taps": bell_draw(key_list[6], (TAPS, FF), TAPS ** -0.5, 3.5, ((1, 8),)),
        "gate_grad_sum": bell_draw(own_keys[7], (D, FF), 1.0, 6.0, ((0, 32), (1, 8)), jnp.float32),
        "up_grad_sum": bell_draw(own_keys[8], (D, FF), 1.0, 6.0, ((0, 32), (1, 8)), jnp.float32),
        "gate_taps_sum": bell_draw(own_keys[9], (TAPS, FF), 1.0, 6.0, ((1, 8),), jnp.float32),
        "up_taps_sum": bell_draw(own_keys[10], (TAPS, FF), 1.0, 6.0, ((1, 8),), jnp.float32),
    }


def causal_mix(values, filter_taps):
    length = values.shape[-2]
    widths = [(0, 0)] * values.ndim
    widths[-2] = (2, 0)
    padded = jnp.pad(values, widths)
    return filter_taps[0] * padded[..., 0:length, :] + filter_taps[1] * padded[..., 1:length + 1, :] + filter_taps[2] * padded[..., 2:length + 2, :]

def mix_back(grads, filter_taps):
    length = grads.shape[-2]
    widths = [(0, 0)] * grads.ndim
    widths[-2] = (0, 2)
    padded = jnp.pad(grads, widths)
    return filter_taps[2] * padded[..., 0:length, :] + filter_taps[1] * padded[..., 1:length + 1, :] + filter_taps[0] * padded[..., 2:length + 2, :]

def tap_products(grads, values):
    length = values.shape[-2]
    widths = [(0, 0)] * values.ndim
    widths[-2] = (2, 0)
    padded = jnp.pad(values, widths)
    axes = tuple(range(values.ndim - 1))
    return jnp.stack([lax.optimization_barrier(jnp.sum(grads * padded[..., offset:offset + length, :], axis=axes)) for offset in range(3)])

def stored(product):
    return lax.optimization_barrier(product.astype(jnp.bfloat16)).astype(jnp.float32)

def reference(late_rows, early_rows, hidden_cot, gate_weight, up_weight, gate_taps, up_taps, gate_grad_sum, up_grad_sum, gate_taps_sum, up_taps_sum):
    rows_scale = TOKENS ** (-0.5)
    gate_filter = gate_taps.astype(jnp.float32)
    up_filter = up_taps.astype(jnp.float32)

    def project(source):
        gate_pre = stored(jnp.dot(source, gate_weight, preferred_element_type=jnp.float32))
        up_pre = stored(jnp.dot(source, up_weight, preferred_element_type=jnp.float32))
        return (gate_pre.reshape(N_FS, TOK_DEV, FF), up_pre.reshape(N_FS, TOK_DEV, FF))
    late_gate, late_up = project(late_rows)
    late_hidden = (jax.nn.gelu(causal_mix(late_gate, gate_filter), approximate=True) * causal_mix(late_up, up_filter)).astype(jnp.bfloat16).reshape(TOKENS, FF)
    early_gate, early_up = project(early_rows)
    gate_mix = causal_mix(early_gate, gate_filter)
    up_mix = causal_mix(early_up, up_filter)
    cotangent = hidden_cot.astype(jnp.float32).reshape(N_FS, TOK_DEV, FF)
    activated, gelu_back = jax.vjp(lambda mixed_value: jax.nn.gelu(mixed_value, approximate=True), gate_mix)
    d_gate_mix = gelu_back(cotangent * up_mix)[0]
    d_up_mix = cotangent * activated
    d_gate_pre = mix_back(d_gate_mix, gate_filter).astype(jnp.bfloat16)
    d_up_pre = mix_back(d_up_mix, up_filter).astype(jnp.bfloat16)
    gate_taps_next = gate_taps_sum + rows_scale * tap_products(d_gate_mix, early_gate)
    up_taps_next = up_taps_sum + rows_scale * tap_products(d_up_mix, early_up)
    flat_gate = d_gate_pre.reshape(TOKENS, FF)
    flat_up = d_up_pre.reshape(TOKENS, FF)
    early_grad = (jnp.dot(flat_gate, gate_weight.T, preferred_element_type=jnp.float32) + jnp.dot(flat_up, up_weight.T, preferred_element_type=jnp.float32)).astype(jnp.bfloat16)
    both_grads = jnp.concatenate([d_gate_pre, d_up_pre], axis=-1)
    blocks = early_rows.reshape(N_FS, TOK_DEV, D)

    def add_device(total, pair):
        block_rows, block_grads = pair
        term = (jnp.dot(block_rows.T, block_grads, preferred_element_type=jnp.float32) * rows_scale).astype(jnp.bfloat16)
        term = lax.optimization_barrier(term)
        return (total + term.astype(jnp.float32), None)
    summed = lax.scan(add_device, jnp.zeros((D, 2 * FF), jnp.float32), (blocks, both_grads))[0]
    return (late_hidden, early_grad, gate_grad_sum + summed[:, :FF], up_grad_sum + summed[:, FF:], gate_taps_next, up_taps_next)
```

```python
import jax
import jax.numpy as jnp
from jax import lax
from jax.experimental import pallas as pl
from jax.experimental.pallas import tpu as pltpu
from jax.sharding import Mesh
from jax.sharding import PartitionSpec as P

FS = ("fs_0", "fs_1")
REP_FS = ("rep", "fs_0", "fs_1")
MESH = pl.DeviceIdType.MESH

NZ, NY, NT = 4, 8, 8
ROWS = 256
LANE = 128
CA, CB = 768, 640
WIDE = CA + CB
HALF = 704
F32, BF16 = jnp.float32, jnp.bfloat16
GELU_K = 0.7978845608028654
GELU_A = 0.044715


def al(v, m):
    return pl.multiple_of(v, m)


def low_lanes(shape):
    return lax.broadcasted_iota(jnp.int32, shape, 1) < 64


def swap_halves(v):
    return pltpu.roll(v, 64, 1)


def row_of(shape):
    return lax.broadcasted_iota(jnp.int32, shape, 0)


def later(v, by):
    return jnp.where(row_of(v.shape) >= by, pltpu.roll(v, by, 0), 0.0)


def sooner(v, by):
    n = v.shape[0]
    return jnp.where(row_of(v.shape) < n - by, pltpu.roll(v, n - by, 0), 0.0)


def gelu_parts(v):
    t = jnp.tanh(GELU_K * (v + GELU_A * v * v * v))
    return 0.5 * v * (1.0 + t), t


def gelu_slope(v, t):
    return 0.5 * (1.0 + t) + 0.5 * v * (1.0 - t * t) * GELU_K * (1.0 + 3.0 * GELU_A * v * v)


def kernel(
    late_ref,
    early_ref,
    cot_ref,
    w_ref,
    taps_ref,
    gsum_ref,
    usum_ref,
    gtsum_ref,
    utsum_ref,
    hid_ref,
    eg_ref,
    gnext_ref,
    unext_ref,
    gtnext_ref,
    utnext_ref,
    wa,
    wb,
    xp,
    xt,
    pre,
    cot,
    dpre,
    dpg,
    snd,
    rcv,
    fin,
    finr,
    dxp,
    dxr,
    egs,
    tsum,
    tzr,
    tys,
    tyr,
    tfr,
    ssem,
    rsem,
):
    rep = lax.axis_index("rep")
    z = lax.axis_index("fs_0")
    y = lax.axis_index("fs_1")
    t = lax.axis_index("tp")
    scale = (NZ * NY * ROWS) ** -0.5

    def ring(k):
        g = lax.rem(rep * NZ + z + 2 * NZ + k, 2 * NZ)
        return {"rep": lax.div(g, NZ), "fs_0": lax.rem(g, NZ)}

    def zdev(k):
        return {"fs_0": lax.rem(z + NZ + k, NZ)}

    def ydev(k):
        return {"fs_1": lax.rem(y + NY + k, NY)}

    def tdev(k):
        return {"tp": lax.rem(t + NT + k, NT)}

    def zat(k):
        return lax.rem(z + NZ + k, NZ)

    def yat(k):
        return lax.rem(y + NY + k, NY)

    peers = [ring(1), ring(-1), ring(2), ring(-2)]
    peers += [zdev(k) for k in range(1, NZ)]
    peers += [ydev(k) for k in range(1, NY)]
    peers += [tdev(k) for k in range(1, NT)]

    barrier = pltpu.get_barrier_semaphore()
    for dev in peers:
        pl.semaphore_signal(barrier, inc=1, device_id=dev, device_id_type=MESH)
    pl.semaphore_wait(barrier, len(peers))

    slots = {}
    sent = []

    def slot(name):
        return slots.setdefault(name, len(slots))

    def copy_of(name, src, dst, dev):
        k = slot(name)
        return pltpu.make_async_remote_copy(
            src_ref=src,
            dst_ref=dst,
            send_sem=ssem.at[k],
            recv_sem=rsem.at[k],
            device_id=dev,
            device_id_type=MESH,
        )

    def send(name, src, dst, dev):
        c = copy_of(name, src, dst, dev)
        c.start()
        sent.append(c)

    def got(name, dst):
        copy_of(name, dst, dst, ydev(1)).wait_recv()

    def wrow(zz, first, n):
        return pl.ds(al(zz * 64 + first, 32), n)

    own = wrow(z, 0, 64)

    a_src = w_ref.at[:, pl.ds(0, CA)]
    send(("a1", 1), a_src, wa.at[y, own], ring(1))
    send(("a1", -1), a_src, wa.at[y, own], ring(-1))
    for h, d in ((0, 1), (1, -1)):
        send(
            ("b1", d, 0, h),
            w_ref.at[pl.ds(32 * h, 32), pl.ds(CA, CB)],
            wb.at[y, wrow(z, 32 * h, 32)],
            ydev(d),
        )
        send(
            ("b1", d, 0, 1 - h),
            w_ref.at[pl.ds(32 * (1 - h), 32), pl.ds(CA, CB)],
            wb.at[y, wrow(z, 32 * (1 - h), 32)],
            ydev(d),
        )
    send(("a1", 2), w_ref.at[pl.ds(0, 32), pl.ds(0, CA)], wa.at[y, wrow(z, 0, 32)], ring(2))
    send(("a1", -2), w_ref.at[pl.ds(32, 32), pl.ds(0, CA)], wa.at[y, wrow(z, 32, 32)], ring(-2))
    b_src = w_ref.at[:, pl.ds(CA, CB)]
    send(("b2", 0, 1), b_src, wb.at[y, own], ring(1))
    send(("b2", 0, -1), b_src, wb.at[y, own], ring(-1))

    wa[y, own, :] = w_ref[:, 0:CA]
    wb[y, own, :] = w_ref[:, CA:WIDE]

    def order_rows(src_ref, first):
        def one(yp, carry):
            for zp in range(2):
                a = src_ref[:, pl.ds(al(2 * zp * 512 + yp * LANE, LANE), LANE)].astype(F32)
                b = src_ref[:, pl.ds(al((2 * zp + 1) * 512 + yp * LANE, LANE), LANE)].astype(F32)
                low = low_lanes(a.shape)
                cols = slice(zp * LANE, (zp + 1) * LANE)
                xp[2 * yp, first : first + ROWS, cols] = jnp.where(low, a, swap_halves(b)).astype(BF16)
                xp[2 * yp + 1, first : first + ROWS, cols] = jnp.where(low, swap_halves(a), b).astype(BF16)
            return carry

        lax.fori_loop(0, NY // 2, one, 0)

    order_rows(early_ref, ROWS)

    def turn(yb, carry):
        xt[yb, 0] = xp[yb, ROWS : 2 * ROWS, :].astype(F32).T.astype(BF16)
        return carry

    lax.fori_loop(0, NY, turn, 0)
    for k in range(1, NZ):
        send(("xz", k), xt.at[t, 0], xt.at[t, k], zdev(-k))

    def a1_take():
        for k in (1, -1):
            got(("a1", k), wa.at[y, wrow(zat(-k), 0, 64)])
        got(("a1", 2), wa.at[y, wrow(zat(2), 0, 32)])
        got(("a1", -2), wa.at[y, wrow(zat(2), 32, 32)])
        for q in range(NZ):
            for d in (1, -1):
                blk = wa.at[y, pl.ds(64 * q, 64)]
                send(("a2", d, 0, q), blk, blk, ydev(d))

    def a2_last(d):
        return (0, 1) if d == 1 else (2, 3)

    def a2_take(s, qs):
        for q in qs:
            for d in (1, -1):
                if s == 4 and q not in a2_last(d):
                    continue
                blk = wa.at[yat(-d * s), pl.ds(64 * q, 64)]
                got(("a2", d, s - 1, q), blk)
                if s < 3 or (s == 3 and q in a2_last(d)):
                    send(("a2", d, s, q), blk, blk, ydev(d))

    def b1_take(s):
        for d in (1, -1):
            mine = 0 if d == 1 else 1
            for h in (mine, 1 - mine):
                if s == 4 and h != mine:
                    continue
                blk = wb.at[yat(-d * s), wrow(z, 32 * h, 32)]
                got(("b1", d, s - 1, h), blk)
                if s < 3 or (s == 3 and h == mine):
                    send(("b1", d, s, h), blk, blk, ydev(d))
        for e in ordinals(s):
            blk = wb.at[yat(-e), own]
            for k in (1, -1):
                send(("b2", e, k), blk, blk, ring(k))

    def ordinals(s):
        return (0,) if s == 0 else ((4,) if s == 4 else (s, -s))

    def b2_take(s):
        for e in ordinals(s):
            for k in (1, -1):
                yb = yat(-e)
                got(("b2", e, k), wb.at[yb, wrow(zat(-k), 0, 64)])
                half = wb.at[yb, wrow(zat(-k), 0 if k == 1 else 32, 32)]
                send(("b2f", e, k), half, half, ring(k))

    def b2f_take(s):
        for e in ordinals(s):
            yb = yat(-e)
            got(("b2f", e, 1), wb.at[yb, wrow(zat(2), 0, 32)])
            got(("b2f", e, -1), wb.at[yb, wrow(zat(2), 32, 32)])

    def project(w, first, width, yb, start):
        rows = xp[yb]

        def tile(c0, n):
            cols = pl.ds(first + c0, n)
            part = jnp.dot(rows, w[yb, :, pl.ds(c0, n)], preferred_element_type=F32)
            pre[:, cols] = part if start else pre[:, cols] + part

        def one(c, carry):
            tile(al(c * 256, 256), 256)
            return carry

        lax.fori_loop(0, width // 256, one, 0)
        if width % 256:
            tile(width - width % 256, width % 256)

    def project_a(s):
        for e in ordinals(s):
            project(wa, 0, CA, yat(-e), s == 0)

    def project_b(s):
        for e in ordinals(s):
            project(wb, CA, CB, yat(-e), s == 0)

    b1_take(1)
    a1_take()
    b2_take(0)
    order_rows(late_ref, 0)
    b1_take(2)
    b2_take(1)
    project_a(0)
    a2_take(1, (0, 1))
    b1_take(3)
    a2_take(1, (2, 3))
    b2_take(2)
    b1_take(4)
    for k in range(1, NZ):
        got(("xz", k), xt.at[t, k])
    mine = xt.at[t, pl.ds(1, 3)]
    for k in (2, 4, 6):
        send(("xx", k), mine, mine, tdev(k))
    pair = {"tp": t + 1 - 2 * lax.rem(t, 2)}
    send(("xc", 0), mine, mine, pair)
    project_a(1)
    a2_take(2, (0, 1))
    b2_take(3)
    a2_take(2, (2, 3))
    b2f_take(0)
    b2f_take(1)
    b2_take(4)
    project_a(2)
    project_b(0)
    a2_take(3, (0, 1))
    a2_take(3, (2, 3))
    project_b(1)
    project_a(3)
    b2f_take(2)
    project_b(2)
    cot[:, 640:CA] = jnp.zeros((ROWS, LANE), BF16)
    cot[:, 0:HALF] = cot_ref[...]
    b2f_take(3)
    project_b(3)
    b2f_take(4)
    project_b(4)
    a2_take(4, range(NZ))
    project_a(4)

    def tap(cols):
        return [taps_ref[j : j + 1, cols] for j in range(3)]

    def mixed(first, cols):
        v = pre[first : first + ROWS, cols].astype(BF16).astype(F32)
        w = tap(cols)
        return v, w[0] * later(v, 2) + w[1] * later(v, 1) + w[2] * v, w

    def back(d, v, w, cols, n):
        dpre[:, cols] = (w[2] * d + w[1] * sooner(d, 1) + w[0] * sooner(d, 2)).astype(BF16)
        q, r = lax.div(n, 3), lax.rem(n, 3)
        spot = pl.ds(al(r * LANE, LANE), LANE)
        for j, u in enumerate((later(v, 2), later(v, 1), v)):
            tsum[q, j : j + 1, spot] = jnp.sum(d * u, axis=0, keepdims=True) * scale

    def tile_cols(n):
        return pl.ds(al(n * LANE, LANE), LANE)

    tsum[...] = jnp.zeros_like(tsum)
    dpre[:, WIDE:] = jnp.zeros((ROWS, LANE), BF16)

    def early_tile(n, carry):
        gc, uc = tile_cols(n), tile_cols(n + 5)
        gv, gm, gw = mixed(ROWS, gc)
        uv, um, uw = mixed(ROWS, uc)
        c = cot[:, gc].astype(F32)
        act, th = gelu_parts(gm)
        back(c * um * gelu_slope(gm, th), gv, gw, gc, n)
        back(c * act, uv, uw, uc, n + 5)
        return carry

    lax.fori_loop(0, 5, early_tile, 0)
    last = slice(1280, 1408)
    mv, mm, mw = mixed(ROWS, last)
    c = cot[:, 640:CA].astype(F32)
    act, th = gelu_parts(mm)
    dg = c * swap_halves(mm) * gelu_slope(mm, th)
    du = swap_halves(c * act)
    back(jnp.where(low_lanes(dg.shape), dg, du), mv, mw, last, 10)

    for i in range(3):
        for k in range(1, NZ):
            send(
                ("dp", i, k),
                dpre.at[:, pl.ds(al((zat(-k) * 3 + i) * LANE, LANE), LANE)],
                dpg.at[i, k],
                zdev(-k),
            )
    for k in range(1, NZ):
        send(("tz", k), tsum.at[zat(-k)], tzr.at[k], zdev(-k))
    for i in range(3):
        dpg[i, 0] = dpre[:, pl.ds(al((z * 3 + i) * LANE, LANE), LANE)]

    def dx(yb, carry):
        nt = (((1,), (1,)), ((), ()))
        v = lax.dot_general(dpre[:, 0:CA], wa[yb], nt, preferred_element_type=F32)
        v = v + lax.dot_general(dpre[:, CA:WIDE], wb[yb], nt, preferred_element_type=F32)
        dxp[:, pl.ds(al(yb * 256, 256), 256)] = v.astype(BF16)
        return carry

    lax.fori_loop(0, NY, dx, 0)

    def strip(tt):
        return pl.ds(al(tt * 32, 32), 32)

    for k in range(1, NT):
        to = lax.rem(t + NT - k, NT)
        send(("dx", k), dxp.at[strip(to)], dxr.at[k], tdev(-k))

    for k in (2, 4, 6):
        row = lax.rem(t + NT - k, NT)
        blk = xt.at[row, pl.ds(1, 3)]
        got(("xx", k), blk)
        send(("xc", k), blk, blk, pair)

    for k in range(1, NZ):
        got(("tz", k), tzr.at[k])
    tys[...] = tsum[z] + tzr[1] + tzr[2] + tzr[3]
    for k in range(1, NY):
        send(("ty", k), tys, tyr.at[k], ydev(-k))

    for k in (0, 2, 4, 6):
        row = lax.rem(t + 1 - 2 * lax.rem(t, 2) + NT - k, NT)
        got(("xc", k), xt.at[row, pl.ds(1, 3)])

    def term(i, yb):
        v = jnp.dot(xt[yb, 0], dpg[i, 0], preferred_element_type=F32)
        for k in range(1, NZ):
            v = v + jnp.dot(xt[yb, k], dpg[i, k], preferred_element_type=F32)
        return v * scale

    def side(d):
        return 0 if d == 1 else 1

    def part(d):
        return pl.ds(0, 128) if d == 1 else pl.ds(128, 128)

    def rs(i, s):
        if s == 0:
            for k in range(1, NZ):
                got(("dp", i, k), dpg.at[i, k])
            v = term(i, yat(4))
            for d in (1, -1):
                buf = snd.at[side(d), i, 0, part(d)]
                buf[...] = (v[0:128] if d == 1 else v[128:256]).astype(BF16)
                send(("rs", i, 0, d), buf, rcv.at[side(d), i, 0, part(d)], ydev(d))
            return
        if s < 4:
            for d in (1, -1):
                snd_f = term(i, yat(d * (4 - s)))
                buf = snd.at[side(d), i, s]
                if s == 1:
                    got(("rs", i, 0, d), rcv.at[side(d), i, 0, part(d)])
                    in_ = rcv[side(d), i, 0, part(d), :].astype(F32)
                    if d == 1:
                        buf[0:128, :] = (snd_f[0:128] + in_).astype(BF16)
                        buf[128:256, :] = snd_f[128:256].astype(BF16)
                    else:
                        buf[0:128, :] = snd_f[0:128].astype(BF16)
                        buf[128:256, :] = (snd_f[128:256] + in_).astype(BF16)
                else:
                    got(("rs", i, s - 1, d), rcv.at[side(d), i, s - 1])
                    buf[...] = (snd_f + rcv[side(d), i, s - 1].astype(F32)).astype(BF16)
                send(("rs", i, s, d), buf, rcv.at[side(d), i, s], ydev(d))
            return
        v = term(i, y)
        for d in (1, -1):
            got(("rs", i, 3, d), rcv.at[side(d), i, 3])
            v = v + rcv[side(d), i, 3].astype(F32)
        fin[i] = v.astype(BF16)
        for k in range(1, NZ):
            send(("fin", i, k), fin.at[i, wrow(zat(-k), 0, 64)], finr.at[k, i], zdev(-k))
        finr[0, i] = fin[i, own, :]

    def dx_reduce():
        for k in range(1, NT):
            got(("dx", k), dxr.at[k])
        v = dxp[strip(t), :].astype(F32)
        for k in range(1, NT):
            v = v + dxr[k].astype(F32)
        for yp in range(NY // 2):
            for zp in range(2):
                a = v[:, 2 * yp * 256 + zp * LANE : 2 * yp * 256 + (zp + 1) * LANE]
                b = v[:, (2 * yp + 1) * 256 + zp * LANE : (2 * yp + 1) * 256 + (zp + 1) * LANE]
                low = low_lanes(a.shape)
                at0 = 2 * zp * 512 + yp * LANE
                egs[:, at0 : at0 + LANE] = jnp.where(low, a, swap_halves(b)).astype(BF16)
                egs[:, at0 + 512 : at0 + 512 + LANE] = jnp.where(low, swap_halves(a), b).astype(BF16)
        for k in range(1, NT):
            send(("eg", k), egs, eg_ref.at[strip(t)], tdev(-k))
        eg_ref[strip(t), :] = egs[...]

    def taps_finish():
        v = tys[...]
        for k in range(1, NY):
            got(("ty", k), tyr.at[k])
            v = v + tyr[k]
        tfr[0] = v
        for k in range(1, NZ):
            send(("tf", k), tfr.at[0], tfr.at[k], zdev(-k))

    def late_tile(n, carry):
        gc = tile_cols(n)
        _, gm, _ = mixed(0, gc)
        _, um, _ = mixed(0, tile_cols(n + 5))
        act, _ = gelu_parts(gm)
        hid_ref[:, gc] = (act * um).astype(BF16)
        return carry

    rs(0, 0)
    lax.fori_loop(0, 5, late_tile, 0)
    _, mm, _ = mixed(0, last)
    act, _ = gelu_parts(mm)
    hid_ref[:, 640:HALF] = (act * swap_halves(mm)).astype(BF16)[:, 0:64]
    rs(0, 1)
    rs(1, 0)
    rs(0, 2)
    rs(1, 1)
    dx_reduce()
    rs(0, 3)
    rs(2, 0)
    rs(1, 2)
    taps_finish()
    rs(2, 1)
    rs(0, 4)
    rs(1, 3)
    rs(2, 2)
    rs(1, 4)
    rs(2, 3)
    rs(2, 4)

    def tile_out(n, v):
        if n < 5:
            cols = slice(n * LANE, (n + 1) * LANE)
            gnext_ref[:, cols] = gsum_ref[:, cols] + v
        elif n < 10:
            cols = slice((n - 5) * LANE, (n - 4) * LANE)
            unext_ref[:, cols] = usum_ref[:, cols] + v
        else:
            gnext_ref[:, 640:HALF] = gsum_ref[:, 640:HALF] + v[:, 0:64]
            unext_ref[:, 640:HALF] = usum_ref[:, 640:HALF] + swap_halves(v)[:, 0:64]

    def taps_out(n, v):
        if n < 5:
            cols = slice(n * LANE, (n + 1) * LANE)
            gtnext_ref[:, cols] = gtsum_ref[:, cols] + v[0:3]
        elif n < 10:
            cols = slice((n - 5) * LANE, (n - 4) * LANE)
            utnext_ref[:, cols] = utsum_ref[:, cols] + v[0:3]
        else:
            gtnext_ref[:, 640:HALF] = gtsum_ref[:, 640:HALF] + v[0:3, 0:64]
            utnext_ref[:, 640:HALF] = utsum_ref[:, 640:HALF] + swap_halves(v)[0:3, 0:64]

    for k in range(1, NZ):
        got(("tf", k), tfr.at[k])
    for k in range(1, NT):
        got(("eg", k), eg_ref.at[strip(lax.rem(t + k, NT))])
    for i in range(3):
        for k in range(1, NZ):
            got(("fin", i, k), finr.at[k, i])
    for n in range(11):
        k = lax.rem(n // 3 + NZ - z, NZ)
        tile_out(n, finr[k, n % 3].astype(F32))
        v = tfr[k]
        taps_out(n, v[:, (n % 3) * LANE : (n % 3 + 1) * LANE])
    for c in sent:
        c.wait_send()


def per_device(
    late_rows,
    early_rows,
    hidden_cot,
    gate_weight,
    up_weight,
    gate_taps,
    up_taps,
    gate_grad_sum,
    up_grad_sum,
    gate_taps_sum,
    up_taps_sum,
):
    def joined(g, u):
        return jnp.concatenate([g[:, :640], u[:, :640], g[:, 640:], u[:, 640:]], axis=1)

    weight = joined(gate_weight, up_weight)
    taps = joined(gate_taps, up_taps).astype(F32)
    vmem = pl.BlockSpec(memory_space=pltpu.VMEM)
    shapes = (
        ((ROWS, HALF), BF16),
        ((ROWS, 2048), BF16),
        ((64, HALF), F32),
        ((64, HALF), F32),
        ((3, HALF), F32),
        ((3, HALF), F32),
    )
    n_sem = 170
    return pl.pallas_call(
        kernel,
        out_shape=[jax.ShapeDtypeStruct(s, d) for s, d in shapes],
        in_specs=[vmem] * 9,
        out_specs=[vmem] * 6,
        scratch_shapes=[
            pltpu.VMEM((NY, 256, CA), BF16),
            pltpu.VMEM((NY, 256, CB), BF16),
            pltpu.VMEM((NY, 2 * ROWS, 256), BF16),
            pltpu.VMEM((NY, NZ, 256, ROWS), BF16),
            pltpu.VMEM((2 * ROWS, WIDE), F32),
            pltpu.VMEM((ROWS, CA), BF16),
            pltpu.VMEM((ROWS, WIDE + LANE), BF16),
            pltpu.VMEM((3, NZ, ROWS, LANE), BF16),
            pltpu.VMEM((2, 3, 4, 256, LANE), BF16),
            pltpu.VMEM((2, 3, 4, 256, LANE), BF16),
            pltpu.VMEM((3, 256, LANE), BF16),
            pltpu.VMEM((NZ, 3, 64, LANE), BF16),
            pltpu.VMEM((ROWS, 2048), BF16),
            pltpu.VMEM((NT, 32, 2048), BF16),
            pltpu.VMEM((32, 2048), BF16),
            pltpu.VMEM((NZ, 8, 384), F32),
            pltpu.VMEM((NZ, 8, 384), F32),
            pltpu.VMEM((8, 384), F32),
            pltpu.VMEM((NY, 8, 384), F32),
            pltpu.VMEM((NZ, 8, 384), F32),
            pltpu.SemaphoreType.DMA((n_sem,)),
            pltpu.SemaphoreType.DMA((n_sem,)),
        ],
        compiler_params=pltpu.CompilerParams(
            collective_id=0, has_side_effects=True, vmem_limit_bytes=60 * 1024 * 1024
        ),
    )(
        late_rows,
        early_rows,
        hidden_cot,
        weight,
        taps,
        gate_grad_sum,
        up_grad_sum,
        gate_taps_sum,
        up_taps_sum,
    )


def solution(mesh):
    split = Mesh(
        mesh.devices.reshape(mesh.shape["rep"], NZ, NY, mesh.shape["tp"]),
        ("rep", "fs_0", "fs_1", "tp"),
    )
    placed = (
        P(REP_FS, None),
        P(REP_FS, None),
        P(REP_FS, "tp"),
        P(FS, "tp"),
        P(FS, "tp"),
        P(None, "tp"),
        P(None, "tp"),
        P(REP_FS, "tp"),
        P(REP_FS, "tp"),
        P("rep", "tp"),
        P("rep", "tp"),
    )
    return jax.shard_map(
        per_device,
        mesh=split,
        in_specs=placed,
        out_specs=(
            P(REP_FS, "tp"),
            P(REP_FS, None),
            P(REP_FS, "tp"),
            P(REP_FS, "tp"),
            P("rep", "tp"),
            P("rep", "tp"),
        ),
        check_vma=False,
    )
```

```python
import jax
import jax.numpy as jnp
from jax import lax
from jax.experimental import pallas as pl
from jax.experimental.pallas import tpu as pltpu
from jax.sharding import Mesh
from jax.sharding import PartitionSpec as P

FS = ("fs_0", "fs_1")
REP_FS = ("rep", "fs_0", "fs_1")
MESH = pl.DeviceIdType.MESH

NZ, NY, NT = 4, 8, 8
ROWS = 256
LANE = 128
CA, CB = 896, 512
WIDE = CA + CB
HALF = 704
GPOS, UPOS = (0, 1, 2, 7, 9), (3, 4, 5, 8, 10)
F32, BF16 = jnp.float32, jnp.bfloat16
GELU_K = 0.7978845608028654
GELU_A = 0.044715


def al(v, m):
    return pl.multiple_of(v, m)


def low_lanes(shape):
    return lax.broadcasted_iota(jnp.int32, shape, 1) < 64


def swap_halves(v):
    return pltpu.roll(v, 64, 1)


def row_of(shape):
    return lax.broadcasted_iota(jnp.int32, shape, 0)


def later(v, by):
    return jnp.where(row_of(v.shape) >= by, pltpu.roll(v, by, 0), 0.0)


def sooner(v, by):
    n = v.shape[0]
    return jnp.where(row_of(v.shape) < n - by, pltpu.roll(v, n - by, 0), 0.0)


def gelu_parts(v):
    t = jnp.tanh(GELU_K * (v + GELU_A * v * v * v))
    return 0.5 * v * (1.0 + t), t


def gelu_slope(v, t):
    return 0.5 * (1.0 + t) + 0.5 * v * (1.0 - t * t) * GELU_K * (1.0 + 3.0 * GELU_A * v * v)


def kernel(
    late_hbm,
    early_hbm,
    cot_hbm,
    gw_hbm,
    uw_hbm,
    gsum_hbm,
    usum_hbm,
    gt_ref,
    ut_ref,
    gtsum_ref,
    utsum_ref,
    hid_ref,
    eg_ref,
    gnext_ref,
    unext_ref,
    gtnext_ref,
    utnext_ref,
    late_ref,
    early_ref,
    cot_ref,
    gw,
    uw,
    gsum_ref,
    usum_ref,
    wmix,
    taps_ref,
    wa,
    wb,
    xe,
    xl,
    xt,
    pre,
    prel,
    cot,
    dpre,
    dpq,
    dpg,
    snd,
    rcv,
    fin,
    finr,
    dxp,
    dxr,
    egs,
    tsum,
    tzr,
    tys,
    tyr,
    tfr,
    lsem,
    ssem,
    rsem,
):
    rep = lax.axis_index("rep")
    z = lax.axis_index("fs_0")
    y = lax.axis_index("fs_1")
    t = lax.axis_index("tp")
    scale = (NZ * NY * ROWS) ** -0.5

    def ring(k):
        g = lax.rem(rep * NZ + z + 2 * NZ + k, 2 * NZ)
        return {"rep": lax.div(g, NZ), "fs_0": lax.rem(g, NZ)}

    def zdev(k):
        return {"fs_0": lax.rem(z + NZ + k, NZ)}

    def ydev(k):
        return {"fs_1": lax.rem(y + NY + k, NY)}

    def tdev(k):
        return {"tp": lax.rem(t + NT + k, NT)}

    def zat(k):
        return lax.rem(z + NZ + k, NZ)

    def yat(k):
        return lax.rem(y + NY + k, NY)

    peers = [ring(1), ring(-1), ring(2), ring(-2)]
    peers += [zdev(k) for k in range(1, NZ)]
    peers += [ydev(k) for k in range(1, NY)]
    peers += [tdev(k) for k in range(1, NT)]

    barrier = pltpu.get_barrier_semaphore()
    for dev in peers:
        pl.semaphore_signal(barrier, inc=1, device_id=dev, device_id_type=MESH)

    pulls = []
    for n, (src, dst) in enumerate(
        (
            (gw_hbm, gw),
            (uw_hbm, uw),
            (early_hbm, early_ref),
            (late_hbm, late_ref),
            (cot_hbm, cot_ref),
            (gsum_hbm, gsum_ref),
            (usum_hbm, usum_ref),
        )
    ):
        c = pltpu.make_async_copy(src, dst, lsem.at[n])
        c.start()
        pulls.append(c)

    slots = {}
    sent = []

    def slot(name):
        return slots.setdefault(name, len(slots))

    def copy_of(name, src, dst, dev):
        k = slot(name)
        return pltpu.make_async_remote_copy(
            src_ref=src,
            dst_ref=dst,
            send_sem=ssem.at[k],
            recv_sem=rsem.at[k],
            device_id=dev,
            device_id_type=MESH,
        )

    def send(name, src, dst, dev):
        c = copy_of(name, src, dst, dev)
        c.start()
        sent.append(c)

    def got(name, dst):
        copy_of(name, dst, dst, ydev(1)).wait_recv()

    def wrow(zz, first, n):
        return pl.ds(al(zz * 64 + first, 32), n)

    own = wrow(z, 0, 64)

    pulls[0].wait()
    pulls[1].wait()
    wmix[:, 0:64] = gw[:, 640:HALF].astype(F32)
    wmix[:, 64:LANE] = uw[:, 640:HALF].astype(F32)
    taps_ref[0:3, 768:832] = gt_ref[:, 640:HALF].astype(F32)
    taps_ref[0:3, 832:CA] = ut_ref[:, 640:HALF].astype(F32)
    wa[y, own, 768:CA] = wmix[...].astype(BF16)
    for n in range(5):
        cols = slice(n * LANE, (n + 1) * LANE)
        for src, tsrc, pos in ((gw, gt_ref, GPOS[n]), (uw, ut_ref, UPOS[n])):
            here = slice(pos * LANE, (pos + 1) * LANE)
            taps_ref[0:3, here] = tsrc[:, cols].astype(F32)
            if pos < 7:
                wa[y, own, here] = src[:, cols]
            else:
                wb[y, own, (pos - 7) * LANE : (pos - 6) * LANE] = src[:, cols]
    pl.semaphore_wait(barrier, len(peers))

    def zrow(q):
        return zat((0, -1, 1, 2)[q])

    def a2_own(q):
        blk = wa.at[y, wrow(zrow(q), 0, 64)]
        for d in (1, -1):
            send(("a2", d, 0, q), blk, blk, ydev(d))

    a_own, b_own = wa.at[y, own], wb.at[y, own]
    for k in (1, -1):
        send(("a1", k), a_own, a_own, ring(k))
    for h, d in ((0, 1), (1, -1), (1, 1), (0, -1)):
        blk = wb.at[y, wrow(z, 32 * h, 32)]
        send(("b1", d, 0, h), blk, blk, ydev(d))
    for h, k in ((0, 2), (1, -2)):
        blk = wa.at[y, wrow(z, 32 * h, 32)]
        send(("a1", k), blk, blk, ring(k))
    a2_own(0)
    for k in (1, -1):
        send(("b2", 0, k), b_own, b_own, ring(k))

    def order_rows(src_ref, dst):
        def one(yp, carry):
            for zp in range(2):
                a = src_ref[:, pl.ds(al(2 * zp * 512 + yp * LANE, LANE), LANE)].astype(F32)
                b = src_ref[:, pl.ds(al((2 * zp + 1) * 512 + yp * LANE, LANE), LANE)].astype(F32)
                low = low_lanes(a.shape)
                cols = slice(zp * LANE, (zp + 1) * LANE)
                dst[2 * yp, :, cols] = jnp.where(low, a, swap_halves(b)).astype(BF16)
                dst[2 * yp + 1, :, cols] = jnp.where(low, swap_halves(a), b).astype(BF16)
            return carry

        lax.fori_loop(0, NY // 2, one, 0)

    pulls[2].wait()
    order_rows(early_ref, xe)

    def turn(yb, carry):
        xt[yb, 0] = xe[yb].astype(F32).T.astype(BF16)
        return carry

    lax.fori_loop(0, NY, turn, 0)

    def x_send(k):
        send(("xz", k), xt.at[t, 0], xt.at[t, k], zdev(-k))

    pair = {"tp": t + 1 - 2 * lax.rem(t, 2)}

    def x_take(j):
        blk = xt.at[t, j]
        got(("xz", j), blk)
        for k in (2, 6):
            send(("xx", k, j), blk, blk, tdev(k))
        send(("xc", 0, j), blk, blk, pair)

    def x_mid(j):
        for k, h in ((2, 0), (6, 128)):
            row = lax.rem(t + NT - k, NT)
            blk = xt.at[row, j]
            got(("xx", k, j), blk)
            half = xt.at[row, j, pl.ds(h, 128)]
            send(("xf", k, j), half, half, tdev(k))
            send(("xc", k, j), blk, blk, pair)

    def x_far(j):
        row = lax.rem(t + 4, NT)
        for k, h in ((2, 0), (6, 128)):
            got(("xf", k, j), xt.at[row, j, pl.ds(h, 128)])
        blk = xt.at[row, j]
        send(("xc", 4, j), blk, blk, pair)

    def x_last():
        for j in range(1, NZ):
            for k in (0, 2, 6, 4):
                row = lax.rem(t + 1 - 2 * lax.rem(t, 2) + NT - k, NT)
                got(("xc", k, j), xt.at[row, j])

    def a1_near():
        for k in (1, -1):
            got(("a1", k), wa.at[y, wrow(zat(-k), 0, 64)])
            a2_own(1 if k == 1 else 2)

    def a1_far():
        got(("a1", 2), wa.at[y, wrow(zat(2), 0, 32)])
        got(("a1", -2), wa.at[y, wrow(zat(2), 32, 32)])
        a2_own(3)

    def a2_last(d):
        return (0, 1) if d == 1 else (2, 3)

    def a2_take(s, qs):
        for q in qs:
            for d in (1, -1):
                if s == 4 and q not in a2_last(d):
                    continue
                blk = wa.at[yat(-d * s), wrow(zrow(q), 0, 64)]
                got(("a2", d, s - 1, q), blk)
                if s < 3 or (s == 3 and q in a2_last(d)):
                    send(("a2", d, s, q), blk, blk, ydev(d))

    def b1_take(s):
        for d in (1, -1):
            mine = 0 if d == 1 else 1
            for h in (mine, 1 - mine):
                if s == 4 and h != mine:
                    continue
                blk = wb.at[yat(-d * s), wrow(z, 32 * h, 32)]
                got(("b1", d, s - 1, h), blk)
                if s < 3 or (s == 3 and h == mine):
                    send(("b1", d, s, h), blk, blk, ydev(d))
        for e in ordinals(s):
            blk = wb.at[yat(-e), own]
            for k in (1, -1):
                send(("b2", e, k), blk, blk, ring(k))

    def ordinals(s):
        return (0,) if s == 0 else ((4,) if s == 4 else (s, -s))

    def b2_take(s):
        for e in ordinals(s):
            for k in (1, -1):
                yb = yat(-e)
                got(("b2", e, k), wb.at[yb, wrow(zat(-k), 0, 64)])
                half = wb.at[yb, wrow(zat(-k), 0 if k == 1 else 32, 32)]
                send(("b2f", e, k), half, half, ring(k))

    def b2f_take(s):
        for e in ordinals(s):
            yb = yat(-e)
            got(("b2f", e, 1), wb.at[yb, wrow(zat(2), 0, 32)])
            got(("b2f", e, -1), wb.at[yb, wrow(zat(2), 32, 32)])

    def project(w, first, width, yb, start):
        rows = xe[yb]

        def tile(c0, n):
            cols = pl.ds(first + c0, n)
            part = jnp.dot(rows, w[yb, :, pl.ds(c0, n)], preferred_element_type=F32)
            pre[:, cols] = part if start else pre[:, cols] + part

        def one(c, carry):
            tile(al(c * 256, 256), 256)
            return carry

        lax.fori_loop(0, width // 256, one, 0)
        if width % 256:
            tile(width - width % 256, width % 256)

    def late_project(w, first, c0, n):
        v = jnp.dot(xl[0], w[0, :, c0 : c0 + n], preferred_element_type=F32)
        for yb in range(1, NY):
            v = v + jnp.dot(xl[yb], w[yb, :, c0 : c0 + n], preferred_element_type=F32)
        prel[:, first + c0 : first + c0 + n] = v

    def project_a(s):
        for e in ordinals(s):
            project(wa, 0, CA, yat(-e), s == 0)

    def project_b(s):
        for e in ordinals(s):
            project(wb, CA, CB, yat(-e), s == 0)

    def turn_cot():
        for n in range(5):
            v = cot_ref[n * LANE : (n + 1) * LANE, :].astype(F32).T
            cot[:, n * LANE : (n + 1) * LANE] = v.astype(BF16)
        cot[:, 640:768] = jnp.zeros((ROWS, LANE), BF16)
        cot[:, 640:HALF] = cot_ref[640:HALF, :].astype(F32).T.astype(BF16)

    def tap(cols):
        return [taps_ref[j : j + 1, cols] for j in range(3)]

    def mixed(src, cols):
        v = src[:, cols].astype(BF16).astype(F32)
        w = tap(cols)
        return v, w[0] * later(v, 2) + w[1] * later(v, 1) + w[2] * v, w

    def back(d, v, w, cols, i, q):
        r = (w[2] * d + w[1] * sooner(d, 1) + w[0] * sooner(d, 2)).astype(BF16)
        dpre[:, cols] = r
        dpq[i, q] = r
        for j, u in enumerate((later(v, 2), later(v, 1), v)):
            tsum[q, i, j : j + 1, :] = jnp.sum(d * u, axis=0, keepdims=True) * scale

    def tile_cols(n):
        return pl.ds(al(n * LANE, LANE), LANE)

    tsum[...] = jnp.zeros_like(tsum)
    dpq[2, 3] = jnp.zeros((ROWS, LANE), BF16)

    def early_pair(n, gpos, upos, i, q):
        gc, uc = tile_cols(gpos), tile_cols(upos)
        gv, gm, gw_ = mixed(pre, gc)
        uv, um, uw_ = mixed(pre, uc)
        c = cot[:, tile_cols(n)].astype(F32)
        act, th = gelu_parts(gm)
        back(c * um * gelu_slope(gm, th), gv, gw_, gc, i, q)
        back(c * act, uv, uw_, uc, i, q + 1)

    def early_b(m, carry):
        early_pair(m + 3, 2 * m + 7, 2 * m + 8, 0, 2 * m)
        return carry

    def early_a(n, carry):
        early_pair(n, n, n + 3, 1 + lax.div(n, 2), lax.rem(2 * n, 4))
        return carry

    last = slice(768, CA)

    def early_last():
        mv, mm, mw = mixed(pre, last)
        c = cot[:, 640:768].astype(F32)
        act, th = gelu_parts(mm)
        dg = c * swap_halves(mm) * gelu_slope(mm, th)
        du = swap_halves(c * act)
        back(jnp.where(low_lanes(dg.shape), dg, du), mv, mw, last, 2, 2)

    def dp_send(i):
        for k in range(1, NZ):
            send(("dp", i, k), dpq.at[i, zat(-k)], dpg.at[i, k], zdev(-k))
        dpg[i, 0] = dpq[i, z]

    b1_take(1)
    a1_near()
    a2_take(1, (0,))
    b2_take(0)
    a1_far()
    x_send(1)
    b1_take(2)
    x_send(2)
    b2_take(1)
    a2_take(1, (1,))
    b1_take(3)
    x_send(3)
    pulls[3].wait()
    order_rows(late_ref, xl)
    a2_take(1, (2,))
    b2_take(2)
    a2_take(1, (3,))
    x_take(1)
    project_a(0)
    b1_take(4)
    project_a(1)
    a2_take(2, (0,))
    b2_take(3)
    x_take(2)
    a2_take(2, (1,))
    x_mid(1)
    b2_take(4)
    a2_take(2, (2,))
    b2f_take(0)
    project_b(0)
    a2_take(2, (3,))
    x_take(3)
    x_mid(2)
    x_far(1)
    project_a(2)
    b2f_take(1)
    project_b(1)
    a2_take(3, (0,))
    b2f_take(2)
    project_b(2)
    x_mid(3)
    x_far(2)
    pulls[4].wait()
    turn_cot()
    a2_take(3, (1,))
    b2f_take(3)
    project_b(3)
    a2_take(3, (2,))
    b2f_take(4)
    project_b(4)
    lax.fori_loop(0, 2, early_b, 0)
    dp_send(0)
    a2_take(3, (3,))
    x_far(3)
    project_a(3)
    a2_take(4, range(NZ))
    project_a(4)
    lax.fori_loop(0, 2, early_a, 0)
    dp_send(1)
    lax.fori_loop(2, 3, early_a, 0)
    early_last()
    for k in range(1, NZ):
        send(("tz", k), tsum.at[zat(-k)], tzr.at[k], zdev(-k))
    dp_send(2)

    def dx(yb, carry):
        nt = (((1,), (1,)), ((), ()))
        v = lax.dot_general(dpre[:, 0:CA], wa[yb], nt, preferred_element_type=F32)
        v = v + lax.dot_general(dpre[:, CA:WIDE], wb[yb], nt, preferred_element_type=F32)
        dxp[:, pl.ds(al(yb * 256, 256), 256)] = v.astype(BF16)
        return carry

    def strip(tt):
        return pl.ds(al(tt * 32, 32), 32)

    def dx_send():
        for k in range(1, NT):
            to = lax.rem(t + NT - k, NT)
            send(("dx", k), dxp.at[strip(to)], dxr.at[k], tdev(-k))

    def taps_first():
        for k in range(1, NZ):
            got(("tz", k), tzr.at[k])
        tys[...] = tsum[z] + tzr[1] + tzr[2] + tzr[3]
        for k in range(1, NY):
            send(("ty", k), tys, tyr.at[k], ydev(-k))

    def term(i, yb):
        v = jnp.dot(xt[yb, 0], dpg[i, 0], preferred_element_type=F32)
        for k in range(1, NZ):
            v = v + jnp.dot(xt[yb, k], dpg[i, k], preferred_element_type=F32)
        return v * scale

    def side(d):
        return 0 if d == 1 else 1

    def part(d):
        return pl.ds(0, 128) if d == 1 else pl.ds(128, 128)

    def rs(i, s):
        if s == 0:
            for k in range(1, NZ):
                got(("dp", i, k), dpg.at[i, k])
            v = term(i, yat(4))
            for d in (1, -1):
                buf = snd.at[side(d), i, 0, part(d)]
                buf[...] = (v[0:128] if d == 1 else v[128:256]).astype(BF16)
                send(("rs", i, 0, d), buf, rcv.at[side(d), i, 0, part(d)], ydev(d))
            return
        if s < 4:
            for d in (1, -1):
                snd_f = term(i, yat(d * (4 - s)))
                buf = snd.at[side(d), i, s]
                if s == 1:
                    got(("rs", i, 0, d), rcv.at[side(d), i, 0, part(d)])
                    in_ = rcv[side(d), i, 0, part(d), :].astype(F32)
                    if d == 1:
                        buf[0:128, :] = (snd_f[0:128] + in_).astype(BF16)
                        buf[128:256, :] = snd_f[128:256].astype(BF16)
                    else:
                        buf[0:128, :] = snd_f[0:128].astype(BF16)
                        buf[128:256, :] = (snd_f[128:256] + in_).astype(BF16)
                else:
                    got(("rs", i, s - 1, d), rcv.at[side(d), i, s - 1])
                    buf[...] = (snd_f + rcv[side(d), i, s - 1].astype(F32)).astype(BF16)
                send(("rs", i, s, d), buf, rcv.at[side(d), i, s], ydev(d))
            return
        v = term(i, y)
        for d in (1, -1):
            got(("rs", i, 3, d), rcv.at[side(d), i, 3])
            v = v + rcv[side(d), i, 3].astype(F32)
        fin[i] = v.astype(BF16)
        for k in range(1, NZ):
            send(("fin", i, k), fin.at[i, wrow(zat(-k), 0, 64)], finr.at[k, i], zdev(-k))
        finr[0, i] = fin[i, own, :]

    def dx_reduce():
        for k in range(1, NT):
            got(("dx", k), dxr.at[k])
        v = dxp[strip(t), :].astype(F32)
        for k in range(1, NT):
            v = v + dxr[k].astype(F32)
        for yp in range(NY // 2):
            for zp in range(2):
                a = v[:, 2 * yp * 256 + zp * LANE : 2 * yp * 256 + (zp + 1) * LANE]
                b = v[:, (2 * yp + 1) * 256 + zp * LANE : (2 * yp + 1) * 256 + (zp + 1) * LANE]
                low = low_lanes(a.shape)
                at0 = 2 * zp * 512 + yp * LANE
                egs[:, at0 : at0 + LANE] = jnp.where(low, a, swap_halves(b)).astype(BF16)
                egs[:, at0 + 512 : at0 + 512 + LANE] = jnp.where(low, swap_halves(a), b).astype(BF16)
        for k in range(1, NT):
            send(("eg", k), egs, eg_ref.at[strip(t)], tdev(-k))
        eg_ref[strip(t), :] = egs[...]

    def taps_finish():
        v = tys[...]
        for k in range(1, NY):
            got(("ty", k), tyr.at[k])
            v = v + tyr[k]
        tfr[0] = v
        for k in range(1, NZ):
            send(("tf", k), tfr.at[0], tfr.at[k], zdev(-k))

    def late_pair(n, gpos, upos):
        _, gm, _ = mixed(prel, tile_cols(gpos))
        _, um, _ = mixed(prel, tile_cols(upos))
        act, _ = gelu_parts(gm)
        hid_ref[tile_cols(n), :] = (act * um).T.astype(BF16)

    def late_b(m, carry):
        late_pair(m + 3, 2 * m + 7, 2 * m + 8)
        return carry

    def late_a(n, carry):
        late_pair(n, n, n + 3)
        return carry

    def late_last():
        _, mm, _ = mixed(prel, last)
        act, _ = gelu_parts(mm)
        hid_ref[640:HALF, :] = (act * swap_halves(mm)).T[0:64].astype(BF16)

    x_last()
    rs(0, 0)
    lax.fori_loop(0, NY, dx, 0)
    dx_send()
    rs(0, 1)
    late_project(wa, 0, 0, 256)
    late_project(wa, 0, 256, 256)
    rs(0, 2)
    rs(1, 0)
    late_project(wa, 0, 512, 256)
    rs(1, 1)
    rs(0, 3)
    dx_reduce()
    late_project(wa, 0, 768, 128)
    rs(2, 0)
    rs(1, 2)
    taps_first()
    rs(0, 4)
    late_project(wb, CA, 0, 256)
    rs(2, 1)
    rs(1, 3)
    late_project(wb, CA, 256, 256)
    rs(2, 2)
    rs(1, 4)
    lax.fori_loop(0, 3, late_a, 0)
    rs(2, 3)
    taps_finish()
    lax.fori_loop(0, 2, late_b, 0)
    late_last()
    rs(2, 4)

    def spread(pos, v, prev, nxt):
        (gs, us), (gn, un) = prev, nxt
        if pos == 6:
            gn[:, 640:HALF] = gs[:, 640:HALF] + v[:, 0:64]
            un[:, 640:HALF] = us[:, 640:HALF] + swap_halves(v)[:, 0:64]
            return
        side_, n = (0, GPOS.index(pos)) if pos in GPOS else (1, UPOS.index(pos))
        cols = slice(n * LANE, (n + 1) * LANE)
        nxt[side_][:, cols] = prev[side_][:, cols] + v

    def tile_out(pos, v):
        spread(pos, v, (gsum_ref, usum_ref), (gnext_ref, unext_ref))

    def taps_out(pos, v):
        if pos == 6:
            gtnext_ref[:, 640:HALF] = gtsum_ref[:, 640:HALF] + v[0:3, 0:64]
            utnext_ref[:, 640:HALF] = utsum_ref[:, 640:HALF] + swap_halves(v)[0:3, 0:64]
            return
        spread(pos, v[0:3], (gtsum_ref, utsum_ref), (gtnext_ref, utnext_ref))

    for k in range(1, NZ):
        got(("tf", k), tfr.at[k])
    for k in range(1, NT):
        got(("eg", k), eg_ref.at[strip(lax.rem(t + k, NT))])
    for i in range(3):
        for k in range(1, NZ):
            got(("fin", i, k), finr.at[k, i])
    pulls[5].wait()
    pulls[6].wait()
    for i, tiles in enumerate(((7, 8, 9, 10), (0, 3, 1, 4), (2, 5, 6))):
        for q, n in enumerate(tiles):
            k = lax.rem(q + NZ - z, NZ)
            tile_out(n, finr[k, i].astype(F32))
            taps_out(n, tfr[k, i])
    for c in sent:
        c.wait_send()


def per_device(
    late_rows,
    early_rows,
    hidden_cot,
    gate_weight,
    up_weight,
    gate_taps,
    up_taps,
    gate_grad_sum,
    up_grad_sum,
    gate_taps_sum,
    up_taps_sum,
):
    vmem = pl.BlockSpec(memory_space=pltpu.VMEM)
    shapes = (
        ((HALF, ROWS), BF16),
        ((ROWS, 2048), BF16),
        ((64, HALF), F32),
        ((64, HALF), F32),
        ((3, HALF), F32),
        ((3, HALF), F32),
    )
    n_sem = 190
    hbm = pl.BlockSpec(memory_space=pltpu.HBM)
    hid, *rest = pl.pallas_call(
        kernel,
        out_shape=[pltpu.VMEM(s, d) for s, d in shapes],
        in_specs=[hbm] * 7 + [vmem] * 4,
        out_specs=[vmem] * 6,
        scratch_shapes=[
            pltpu.VMEM((ROWS, 2048), BF16),
            pltpu.VMEM((ROWS, 2048), BF16),
            pltpu.VMEM((HALF, ROWS), BF16),
            pltpu.VMEM((64, HALF), BF16),
            pltpu.VMEM((64, HALF), BF16),
            pltpu.VMEM((64, HALF), F32),
            pltpu.VMEM((64, HALF), F32),
            pltpu.VMEM((64, LANE), F32),
            pltpu.VMEM((8, WIDE), F32),
            pltpu.VMEM((NY, 256, CA), BF16),
            pltpu.VMEM((NY, 256, CB), BF16),
            pltpu.VMEM((NY, ROWS, 256), BF16),
            pltpu.VMEM((NY, ROWS, 256), BF16),
            pltpu.VMEM((NY, NZ, 256, ROWS), BF16),
            pltpu.VMEM((ROWS, WIDE), F32),
            pltpu.VMEM((ROWS, WIDE), F32),
            pltpu.VMEM((ROWS, 768), BF16),
            pltpu.VMEM((ROWS, WIDE), BF16),
            pltpu.VMEM((3, NZ, ROWS, LANE), BF16),
            pltpu.VMEM((3, NZ, ROWS, LANE), BF16),
            pltpu.VMEM((2, 3, 4, 256, LANE), BF16),
            pltpu.VMEM((2, 3, 4, 256, LANE), BF16),
            pltpu.VMEM((3, 256, LANE), BF16),
            pltpu.VMEM((NZ, 3, 64, LANE), BF16),
            pltpu.VMEM((ROWS, 2048), BF16),
            pltpu.VMEM((NT, 32, 2048), BF16),
            pltpu.VMEM((32, 2048), BF16),
            pltpu.VMEM((NZ, 3, 8, LANE), F32),
            pltpu.VMEM((NZ, 3, 8, LANE), F32),
            pltpu.VMEM((3, 8, LANE), F32),
            pltpu.VMEM((NY, 3, 8, LANE), F32),
            pltpu.VMEM((NZ, 3, 8, LANE), F32),
            pltpu.SemaphoreType.DMA((7,)),
            pltpu.SemaphoreType.DMA((n_sem,)),
            pltpu.SemaphoreType.DMA((n_sem,)),
        ],
        compiler_params=pltpu.CompilerParams(
            collective_id=0, has_side_effects=True, vmem_limit_bytes=57000 * 1024
        ),
    )(
        late_rows,
        early_rows,
        hidden_cot.T,
        gate_weight,
        up_weight,
        gate_grad_sum,
        up_grad_sum,
        gate_taps,
        up_taps,
        gate_taps_sum,
        up_taps_sum,
    )
    return (hid.T, *rest)


def solution(mesh):
    split = Mesh(
        mesh.devices.reshape(mesh.shape["rep"], NZ, NY, mesh.shape["tp"]),
        ("rep", "fs_0", "fs_1", "tp"),
    )
    placed = (
        P(REP_FS, None),
        P(REP_FS, None),
        P(REP_FS, "tp"),
        P(FS, "tp"),
        P(FS, "tp"),
        P(None, "tp"),
        P(None, "tp"),
        P(REP_FS, "tp"),
        P(REP_FS, "tp"),
        P("rep", "tp"),
        P("rep", "tp"),
    )
    return jax.shard_map(
        per_device,
        mesh=split,
        in_specs=placed,
        out_specs=(
            P(REP_FS, "tp"),
            P(REP_FS, None),
            P(REP_FS, "tp"),
            P(REP_FS, "tp"),
            P("rep", "tp"),
            P("rep", "tp"),
        ),
        check_vma=False,
    )
```

```python
import jax
import jax.numpy as jnp
from jax import lax
from jax.experimental import pallas as pl
from jax.experimental.pallas import tpu as pltpu
from jax.sharding import Mesh
from jax.sharding import PartitionSpec as P

FS = ("fs_0", "fs_1")
REP_FS = ("rep", "fs_0", "fs_1")
MESH = pl.DeviceIdType.MESH

NZ, NY, NT = 4, 8, 8
ROWS = 256
LANE = 128
CA, CC, CB = 512, 384, 512
AC = CA + CC
WIDE = AC + CB
HALF = 704
GPOS, UPOS = (0, 2, 4, 7, 9), (1, 3, 5, 8, 10)
F32, BF16 = jnp.float32, jnp.bfloat16
GELU_K = 0.7978845608028654
GELU_A = 0.044715


def al(v, m):
    return pl.multiple_of(v, m)


def low_lanes(shape):
    return lax.broadcasted_iota(jnp.int32, shape, 1) < 64


def swap_halves(v):
    return pltpu.roll(v, 64, 1)


def row_of(shape):
    return lax.broadcasted_iota(jnp.int32, shape, 0)


def later(v, by):
    return jnp.where(row_of(v.shape) >= by, pltpu.roll(v, by, 0), 0.0)


def sooner(v, by):
    n = v.shape[0]
    return jnp.where(row_of(v.shape) < n - by, pltpu.roll(v, n - by, 0), 0.0)


def gelu_parts(v):
    t = jnp.tanh(GELU_K * (v + GELU_A * v * v * v))
    return 0.5 * v * (1.0 + t), t


def gelu_slope(v, t):
    return 0.5 * (1.0 + t) + 0.5 * v * (1.0 - t * t) * GELU_K * (1.0 + 3.0 * GELU_A * v * v)


def kernel(
    late_hbm,
    early_hbm,
    cot_hbm,
    gw_hbm,
    uw_hbm,
    gsum_hbm,
    usum_hbm,
    gt_hbm,
    ut_hbm,
    gtsum_hbm,
    utsum_hbm,
    hid_ref,
    eg_ref,
    gnext_ref,
    unext_ref,
    gtnext_ref,
    utnext_ref,
    late_ref,
    early_ref,
    cot_ref,
    gw,
    uw,
    gsum_ref,
    usum_ref,
    gt_ref,
    ut_ref,
    gtsum_ref,
    utsum_ref,
    wmix,
    taps_ref,
    wa,
    wc,
    wb,
    xe,
    xl,
    xt,
    pre,
    prel,
    cot,
    dpre,
    dpq,
    dpg,
    snd,
    rcv,
    fin,
    finr,
    dxp,
    dxc,
    dxs,
    dxr,
    egs,
    tsum,
    tzr,
    tys,
    tyr,
    tfr,
    lsem,
    ssem,
    rsem,
):
    rep = lax.axis_index("rep")
    z = lax.axis_index("fs_0")
    y = lax.axis_index("fs_1")
    t = lax.axis_index("tp")
    scale = (NZ * NY * ROWS) ** -0.5

    def ring(k):
        g = lax.rem(rep * NZ + z + 2 * NZ + k, 2 * NZ)
        return {"rep": lax.div(g, NZ), "fs_0": lax.rem(g, NZ)}

    def zdev(k):
        return {"fs_0": lax.rem(z + NZ + k, NZ)}

    def ydev(k):
        return {"fs_1": lax.rem(y + NY + k, NY)}

    def tdev(k):
        return {"tp": lax.rem(t + NT + k, NT)}

    def zat(k):
        return lax.rem(z + NZ + k, NZ)

    def yat(k):
        return lax.rem(y + NY + k, NY)

    peers = [ring(1), ring(-1), ring(2), ring(-2)]
    peers += [zdev(k) for k in range(1, NZ)]
    peers += [ydev(k) for k in range(1, NY)]
    peers += [tdev(k) for k in range(1, NT)]

    barrier = pltpu.get_barrier_semaphore()
    for dev in peers:
        pl.semaphore_signal(barrier, inc=1, device_id=dev, device_id_type=MESH)

    pulls = []
    for n, (src, dst) in enumerate(
        (
            (gw_hbm, gw),
            (uw_hbm, uw),
            (early_hbm, early_ref),
            (late_hbm, late_ref),
            (cot_hbm, cot_ref),
            (gsum_hbm, gsum_ref),
            (usum_hbm, usum_ref),
            (gt_hbm, gt_ref),
            (ut_hbm, ut_ref),
            (gtsum_hbm, gtsum_ref),
            (utsum_hbm, utsum_ref),
        )
    ):
        c = pltpu.make_async_copy(src, dst, lsem.at[n])
        c.start()
        pulls.append(c)

    slots = {}
    sent = []

    def slot(name):
        return slots.setdefault(name, len(slots))

    def copy_of(name, src, dst, dev):
        k = slot(name)
        return pltpu.make_async_remote_copy(
            src_ref=src,
            dst_ref=dst,
            send_sem=ssem.at[k],
            recv_sem=rsem.at[k],
            device_id=dev,
            device_id_type=MESH,
        )

    def send(name, src, dst, dev):
        c = copy_of(name, src, dst, dev)
        c.start()
        sent.append(c)

    def got(name, dst):
        copy_of(name, dst, dst, ydev(1)).wait_recv()

    def wrow(zz, first, n):
        return pl.ds(al(zz * 64 + first, 32), n)

    own = wrow(z, 0, 64)

    pulls[0].wait()
    pulls[1].wait()
    wmix[:, 0:64] = gw[:, 640:HALF].astype(F32)
    wmix[:, 64:LANE] = uw[:, 640:HALF].astype(F32)
    wc[y, own, 256:CC] = wmix[...].astype(BF16)
    for n in range(5):
        cols = slice(n * LANE, (n + 1) * LANE)
        for src, pos in ((gw, GPOS[n]), (uw, UPOS[n])):
            here = slice(pos * LANE, (pos + 1) * LANE)
            if pos < 4:
                wa[y, own, here] = src[:, cols]
            elif pos < 7:
                wc[y, own, (pos - 4) * LANE : (pos - 3) * LANE] = src[:, cols]
            else:
                wb[y, own, (pos - 7) * LANE : (pos - 6) * LANE] = src[:, cols]
    pl.semaphore_wait(barrier, len(peers))

    def zrow(q):
        return zat((0, -1, 1, 2)[q])

    wide = {"a": wa, "c": wc}

    def a2_own(p, q):
        blk = wide[p].at[y, wrow(zrow(q), 0, 64)]
        for d in (1, -1):
            send(("a2", p, d, 0, q), blk, blk, ydev(d))

    def a1_send(p, near):
        if near:
            blk = wide[p].at[y, own]
            for k in (1, -1):
                send(("a1", p, k), blk, blk, ring(k))
            return
        for h, k in ((0, 2), (1, -2)):
            blk = wide[p].at[y, wrow(z, 32 * h, 32)]
            send(("a1", p, k), blk, blk, ring(k))

    b_own = wb.at[y, own]
    a1_send("a", True)
    for h, d in ((0, 1), (1, -1), (1, 1), (0, -1)):
        blk = wb.at[y, wrow(z, 32 * h, 32)]
        send(("b1", d, 0, h), blk, blk, ydev(d))
    a1_send("a", False)
    a2_own("a", 0)
    for k in (1, -1):
        send(("b2", 0, k), b_own, b_own, ring(k))
    a1_send("c", True)
    a1_send("c", False)

    def order_rows(src_ref, dst):
        def one(yp, carry):
            for zp in range(2):
                a = src_ref[:, pl.ds(al(2 * zp * 512 + yp * LANE, LANE), LANE)].astype(F32)
                b = src_ref[:, pl.ds(al((2 * zp + 1) * 512 + yp * LANE, LANE), LANE)].astype(F32)
                low = low_lanes(a.shape)
                cols = slice(zp * LANE, (zp + 1) * LANE)
                dst[2 * yp, :, cols] = jnp.where(low, a, swap_halves(b)).astype(BF16)
                dst[2 * yp + 1, :, cols] = jnp.where(low, swap_halves(a), b).astype(BF16)
            return carry

        lax.fori_loop(0, NY // 2, one, 0)

    pulls[2].wait()
    order_rows(early_ref, xe)

    def turn(yb, carry):
        xt[yb, 0] = xe[yb].astype(F32).T.astype(BF16)
        return carry

    lax.fori_loop(0, NY, turn, 0)

    def x_send(k):
        send(("xz", k), xt.at[t, 0], xt.at[t, k], zdev(-k))

    pair = {"tp": t + 1 - 2 * lax.rem(t, 2)}

    def x_take(j):
        blk = xt.at[t, j]
        got(("xz", j), blk)
        for k in (2, 6):
            send(("xx", k, j), blk, blk, tdev(k))
        send(("xc", 0, j), blk, blk, pair)

    def x_mid(j):
        for k, h in ((2, 0), (6, 128)):
            row = lax.rem(t + NT - k, NT)
            blk = xt.at[row, j]
            got(("xx", k, j), blk)
            half = xt.at[row, j, pl.ds(h, 128)]
            send(("xf", k, j), half, half, tdev(k))
            send(("xc", k, j), blk, blk, pair)

    def x_far(j):
        row = lax.rem(t + 4, NT)
        for k, h in ((2, 0), (6, 128)):
            got(("xf", k, j), xt.at[row, j, pl.ds(h, 128)])
        blk = xt.at[row, j]
        send(("xc", 4, j), blk, blk, pair)

    def x_last():
        for j in range(1, NZ):
            for k in (0, 2, 6, 4):
                row = lax.rem(t + 1 - 2 * lax.rem(t, 2) + NT - k, NT)
                got(("xc", k, j), xt.at[row, j])

    def a1_near(p):
        for k in (1, -1):
            got(("a1", p, k), wide[p].at[y, wrow(zat(-k), 0, 64)])

    def a1_far(p):
        got(("a1", p, 2), wide[p].at[y, wrow(zat(2), 0, 32)])
        got(("a1", p, -2), wide[p].at[y, wrow(zat(2), 32, 32)])

    def a2_last(d):
        return (0, 1) if d == 1 else (2, 3)

    def a2_take(p, s, qs):
        for q in qs:
            for d in (1, -1):
                if s == 4 and q not in a2_last(d):
                    continue
                blk = wide[p].at[yat(-d * s), wrow(zrow(q), 0, 64)]
                got(("a2", p, d, s - 1, q), blk)
                if s < 3 or (s == 3 and q in a2_last(d)):
                    send(("a2", p, d, s, q), blk, blk, ydev(d))

    def b1_take(s):
        for d in (1, -1):
            mine = 0 if d == 1 else 1
            for h in (mine, 1 - mine):
                if s == 4 and h != mine:
                    continue
                blk = wb.at[yat(-d * s), wrow(z, 32 * h, 32)]
                got(("b1", d, s - 1, h), blk)
                if s < 3 or (s == 3 and h == mine):
                    send(("b1", d, s, h), blk, blk, ydev(d))
        for e in ordinals(s):
            blk = wb.at[yat(-e), own]
            for k in (1, -1):
                send(("b2", e, k), blk, blk, ring(k))

    def ordinals(s):
        return (0,) if s == 0 else ((4,) if s == 4 else (s, -s))

    def b2_take(s):
        for e in ordinals(s):
            for k in (1, -1):
                yb = yat(-e)
                got(("b2", e, k), wb.at[yb, wrow(zat(-k), 0, 64)])
                half = wb.at[yb, wrow(zat(-k), 0 if k == 1 else 32, 32)]
                send(("b2f", e, k), half, half, ring(k))

    def b2f_take(s):
        for e in ordinals(s):
            yb = yat(-e)
            got(("b2f", e, 1), wb.at[yb, wrow(zat(2), 0, 32)])
            got(("b2f", e, -1), wb.at[yb, wrow(zat(2), 32, 32)])

    def project(w, first, width, yb, start):
        rows = xe[yb]

        def tile(c0, n):
            cols = pl.ds(first + c0, n)
            part = jnp.dot(rows, w[yb, :, pl.ds(c0, n)], preferred_element_type=F32)
            pre[:, cols] = part if start else pre[:, cols] + part

        def one(c, carry):
            tile(al(c * 256, 256), 256)
            return carry

        lax.fori_loop(0, width // 256, one, 0)
        if width % 256:
            tile(width - width % 256, width % 256)

    def late_project(w, first, c0, n):
        v = jnp.dot(xl[0], w[0, :, c0 : c0 + n], preferred_element_type=F32)
        for yb in range(1, NY):
            v = v + jnp.dot(xl[yb], w[yb, :, c0 : c0 + n], preferred_element_type=F32)
        prel[:, first + c0 : first + c0 + n] = v

    def project_a(s):
        for e in ordinals(s):
            project(wa, 0, CA, yat(-e), s == 0)

    def project_c(s):
        for e in ordinals(s):
            project(wc, CA, CC, yat(-e), s == 0)

    def project_b(s):
        for e in ordinals(s):
            project(wb, AC, CB, yat(-e), s == 0)

    def join_taps():
        for n in range(7, 11):
            pulls[n].wait()
        for n in range(5):
            cols = slice(n * LANE, (n + 1) * LANE)
            for src, pos in ((gt_ref, GPOS[n]), (ut_ref, UPOS[n])):
                taps_ref[0:3, pos * LANE : (pos + 1) * LANE] = src[:, cols].astype(F32)
        taps_ref[0:3, 768:832] = gt_ref[:, 640:HALF].astype(F32)
        taps_ref[0:3, 832:AC] = ut_ref[:, 640:HALF].astype(F32)

    def turn_cot():
        for n in range(5):
            v = cot_ref[n * LANE : (n + 1) * LANE, :].astype(F32).T
            cot[:, n * LANE : (n + 1) * LANE] = v.astype(BF16)
        cot[:, 640:768] = jnp.zeros((ROWS, LANE), BF16)
        cot[:, 640:HALF] = cot_ref[640:HALF, :].astype(F32).T.astype(BF16)

    def tap(cols):
        return [taps_ref[j : j + 1, cols] for j in range(3)]

    def mixed(src, cols):
        v = src[:, cols].astype(BF16).astype(F32)
        w = tap(cols)
        return v, w[0] * later(v, 2) + w[1] * later(v, 1) + w[2] * v, w

    def back(d, v, w, cols, i, q):
        r = (w[2] * d + w[1] * sooner(d, 1) + w[0] * sooner(d, 2)).astype(BF16)
        dpre[:, cols] = r
        dpq[i, q] = r
        for j, u in enumerate((later(v, 2), later(v, 1), v)):
            tsum[q, i, j : j + 1, :] = jnp.sum(d * u, axis=0, keepdims=True) * scale

    def tile_cols(n):
        return pl.ds(al(n * LANE, LANE), LANE)

    tsum[...] = jnp.zeros_like(tsum)
    dpq[2, 3] = jnp.zeros((ROWS, LANE), BF16)

    def early_pair(n, gpos, upos, i, q):
        gc, uc = tile_cols(gpos), tile_cols(upos)
        gv, gm, gw_ = mixed(pre, gc)
        uv, um, uw_ = mixed(pre, uc)
        c = cot[:, tile_cols(n)].astype(F32)
        act, th = gelu_parts(gm)
        back(c * um * gelu_slope(gm, th), gv, gw_, gc, i, q)
        back(c * act, uv, uw_, uc, i, q + 1)

    def early_a(n, carry):
        early_pair(n, 2 * n, 2 * n + 1, 0, 2 * n)
        return carry

    def early_b(m, carry):
        early_pair(m + 3, 2 * m + 7, 2 * m + 8, 1, 2 * m)
        return carry

    last = slice(768, AC)

    def early_c():
        early_pair(2, 4, 5, 2, 0)
        mv, mm, mw = mixed(pre, last)
        c = cot[:, 640:768].astype(F32)
        act, th = gelu_parts(mm)
        dg = c * swap_halves(mm) * gelu_slope(mm, th)
        du = swap_halves(c * act)
        back(jnp.where(low_lanes(dg.shape), dg, du), mv, mw, last, 2, 2)
        for k in range(1, NZ):
            send(("tz", k), tsum.at[zat(-k)], tzr.at[k], zdev(-k))

    def dp_send(i):
        for k in range(1, NZ):
            send(("dp", i, k), dpq.at[i, zat(-k)], dpg.at[i, k], zdev(-k))
        dpg[i, 0] = dpq[i, z]

    def dx(yb, carry):
        nt = (((1,), (1,)), ((), ()))
        v = lax.dot_general(dpre[:, 0:CA], wa[yb], nt, preferred_element_type=F32)
        v = v + lax.dot_general(dpre[:, CA:AC], wc[yb], nt, preferred_element_type=F32)
        v = v + lax.dot_general(dpre[:, AC:WIDE], wb[yb], nt, preferred_element_type=F32)
        dxp[:, pl.ds(al(yb * 256, 256), 256)] = v.astype(BF16)
        return carry

    def strip(tt):
        return pl.ds(al(tt * 32, 32), 32)

    core = lax.rem(t, 2)

    def dx_send():
        for x in range(4):
            send(("dc", x), dxp.at[strip(2 * x + 1 - core)], dxc.at[x], pair)

    def dx_pair():
        for x in range(4):
            got(("dc", x), dxc.at[x])
            v = dxp[strip(2 * x + core), :].astype(F32) + dxc[x].astype(F32)
            dxs[x] = v.astype(BF16)
        for k in (2, 6, 4):
            to = lax.div(lax.rem(t + NT - k, NT), 2)
            send(("dx", k), dxs.at[to], dxr.at[k // 2], tdev(-k))

    def taps_first():
        for k in range(1, NZ):
            got(("tz", k), tzr.at[k])
        tys[...] = tsum[z] + tzr[1] + tzr[2] + tzr[3]
        for k in range(1, NY):
            send(("ty", k), tys, tyr.at[k], ydev(-k))

    def term(i, yb):
        v = jnp.dot(xt[yb, 0], dpg[i, 0], preferred_element_type=F32)
        for k in range(1, NZ):
            v = v + jnp.dot(xt[yb, k], dpg[i, k], preferred_element_type=F32)
        return v * scale

    def side(d):
        return 0 if d == 1 else 1

    def part(d):
        return pl.ds(0, 128) if d == 1 else pl.ds(128, 128)

    def rs(i, s):
        if s == 0:
            for k in range(1, NZ):
                got(("dp", i, k), dpg.at[i, k])
            for d in (1, -1):
                buf = snd.at[side(d), i, 0]
                buf[...] = term(i, yat(3 * d)).astype(BF16)
                send(("rs", i, 0, d), buf, rcv.at[side(d), i, 0], ydev(d))
            v = term(i, yat(4))
            for d in (1, -1):
                buf = snd.at[side(d), i, 3, part(d)]
                buf[...] = (v[0:128] if d == 1 else v[128:256]).astype(BF16)
                send(("rs", i, 3, d), buf, rcv.at[side(d), i, 3, part(d)], ydev(2 * d))
            return
        if s < 3:
            for d in (1, -1):
                v = term(i, yat(d * (3 - s)))
                got(("rs", i, s - 1, d), rcv.at[side(d), i, s - 1])
                v = v + rcv[side(d), i, s - 1].astype(F32)
                buf = snd.at[side(d), i, s]
                if s == 1:
                    far = rcv.at[side(d), i, 3, part(d)]
                    got(("rs", i, 3, d), far)
                    w = far[...].astype(F32)
                    if d == 1:
                        buf[0:128, :] = (v[0:128] + w).astype(BF16)
                        buf[128:256, :] = v[128:256].astype(BF16)
                    else:
                        buf[0:128, :] = v[0:128].astype(BF16)
                        buf[128:256, :] = (v[128:256] + w).astype(BF16)
                else:
                    buf[...] = v.astype(BF16)
                send(("rs", i, s, d), buf, rcv.at[side(d), i, s], ydev(d))
            return
        v = term(i, y)
        for d in (1, -1):
            got(("rs", i, 2, d), rcv.at[side(d), i, 2])
            v = v + rcv[side(d), i, 2].astype(F32)
        fin[i] = v.astype(BF16)
        for k in range(1, NZ):
            send(("fin", i, k), fin.at[i, wrow(zat(-k), 0, 64)], finr.at[k, i], zdev(-k))
        finr[0, i] = fin[i, own, :]

    def dx_reduce():
        v = dxs[lax.div(t, 2)].astype(F32)
        for k in (2, 6, 4):
            got(("dx", k), dxr.at[k // 2])
            v = v + dxr[k // 2].astype(F32)
        for yp in range(NY // 2):
            for zp in range(2):
                a = v[:, 2 * yp * 256 + zp * LANE : 2 * yp * 256 + (zp + 1) * LANE]
                b = v[:, (2 * yp + 1) * 256 + zp * LANE : (2 * yp + 1) * 256 + (zp + 1) * LANE]
                low = low_lanes(a.shape)
                at0 = 2 * zp * 512 + yp * LANE
                egs[:, at0 : at0 + LANE] = jnp.where(low, a, swap_halves(b)).astype(BF16)
                egs[:, at0 + 512 : at0 + 512 + LANE] = jnp.where(low, swap_halves(a), b).astype(BF16)
        for k in (2, 6, 4):
            send(("eg", k), egs, eg_ref.at[strip(t)], tdev(k))
        send(("ec", 0), egs, eg_ref.at[strip(t)], pair)
        eg_ref[strip(t), :] = egs[...]

    def eg_cross():
        for k in (2, 6, 4):
            here = eg_ref.at[strip(lax.rem(t + NT - k, NT))]
            got(("eg", k), here)
            send(("ec", k), here, here, pair)

    def eg_last():
        for k in (0, 2, 6, 4):
            row = lax.rem(t + 1 - 2 * lax.rem(t, 2) + NT - k, NT)
            got(("ec", k), eg_ref.at[strip(row)])

    def taps_finish():
        v = tys[...]
        for k in range(1, NY):
            got(("ty", k), tyr.at[k])
            v = v + tyr[k]
        tfr[0] = v
        for k in range(1, NZ):
            send(("tf", k), tfr.at[0], tfr.at[k], zdev(-k))

    def late_pair(n, gpos, upos):
        _, gm, _ = mixed(prel, tile_cols(gpos))
        _, um, _ = mixed(prel, tile_cols(upos))
        act, _ = gelu_parts(gm)
        hid_ref[tile_cols(n), :] = (act * um).T.astype(BF16)

    def late_a(n, carry):
        late_pair(n, 2 * n, 2 * n + 1)
        return carry

    def late_b(m, carry):
        late_pair(m + 3, 2 * m + 7, 2 * m + 8)
        return carry

    def late_c():
        late_pair(2, 4, 5)
        _, mm, _ = mixed(prel, last)
        act, _ = gelu_parts(mm)
        hid_ref[640:HALF, :] = (act * swap_halves(mm)).T[0:64].astype(BF16)

    b1_take(1)
    a1_near("a")
    a2_own("a", 1)
    a2_own("a", 2)
    a2_take("a", 1, (0,))
    a1_far("a")
    a2_own("a", 3)
    b2_take(0)
    x_send(1)
    a2_take("a", 1, (1,))
    b1_take(2)
    x_send(2)
    a2_take("a", 1, (2,))
    a2_take("a", 1, (3,))
    b2_take(1)
    x_send(3)
    pulls[3].wait()
    order_rows(late_ref, xl)
    b1_take(3)
    a2_take("a", 2, (0, 1))
    project_a(0)
    a2_take("a", 2, (2, 3))
    b2_take(2)
    b1_take(4)
    x_take(1)
    a1_near("c")
    a1_far("c")
    a2_take("a", 3, (0,))
    a2_own("c", 0)
    project_a(1)
    a2_take("a", 3, (1,))
    a2_own("c", 1)
    a2_take("a", 3, (2,))
    a2_own("c", 2)
    a2_take("a", 3, (3,))
    a2_own("c", 3)
    x_take(2)
    project_a(2)
    a2_take("a", 4, range(NZ))
    a2_take("c", 1, (0,))
    b2_take(3)
    project_a(3)
    a2_take("c", 1, (1,))
    x_mid(1)
    pulls[4].wait()
    turn_cot()
    join_taps()
    a2_take("c", 1, (2,))
    project_a(4)
    lax.fori_loop(0, 2, early_a, 0)
    dp_send(0)
    a2_take("c", 1, (3,))
    b2_take(4)
    x_take(3)
    a2_take("c", 2, (0,))
    x_mid(2)
    x_far(1)
    a2_take("c", 2, (1,))
    b2f_take(0)
    project_b(0)
    b2f_take(1)
    project_b(1)
    a2_take("c", 2, (2, 3))
    b2f_take(2)
    project_b(2)
    a2_take("c", 3, (0,))
    x_mid(3)
    x_far(2)
    project_c(0)
    a2_take("c", 3, (1,))
    b2f_take(3)
    project_b(3)
    a2_take("c", 3, (2, 3))
    b2f_take(4)
    project_b(4)
    lax.fori_loop(0, 2, early_b, 0)
    dp_send(1)
    project_c(1)
    project_c(2)
    project_c(3)
    x_far(3)
    a2_take("c", 4, range(NZ))
    project_c(4)
    early_c()
    dp_send(2)
    x_last()
    rs(0, 0)
    lax.fori_loop(0, NY, dx, 0)
    dx_send()
    rs(0, 1)
    rs(1, 0)
    dx_pair()
    taps_first()
    late_project(wa, 0, 0, 256)
    rs(0, 2)
    rs(1, 1)
    rs(2, 0)
    late_project(wa, 0, 256, 256)
    rs(0, 3)
    rs(1, 2)
    rs(2, 1)
    dx_reduce()
    late_project(wc, CA, 0, 256)
    late_project(wc, CA, 256, 128)
    rs(1, 3)
    rs(2, 2)
    late_project(wb, AC, 0, 256)
    late_project(wb, AC, 256, 256)
    taps_finish()
    eg_cross()
    lax.fori_loop(0, 2, late_a, 0)
    rs(2, 3)
    lax.fori_loop(0, 2, late_b, 0)
    late_c()

    def spread(pos, v, prev, nxt):
        (gs, us), (gn, un) = prev, nxt
        if pos == 6:
            gn[:, 640:HALF] = gs[:, 640:HALF] + v[:, 0:64]
            un[:, 640:HALF] = us[:, 640:HALF] + swap_halves(v)[:, 0:64]
            return
        side_, n = (0, GPOS.index(pos)) if pos in GPOS else (1, UPOS.index(pos))
        cols = slice(n * LANE, (n + 1) * LANE)
        nxt[side_][:, cols] = prev[side_][:, cols] + v

    def tile_out(pos, v):
        spread(pos, v, (gsum_ref, usum_ref), (gnext_ref, unext_ref))

    def taps_out(pos, v):
        if pos == 6:
            gtnext_ref[:, 640:HALF] = gtsum_ref[:, 640:HALF] + v[0:3, 0:64]
            utnext_ref[:, 640:HALF] = utsum_ref[:, 640:HALF] + swap_halves(v)[0:3, 0:64]
            return
        spread(pos, v[0:3], (gtsum_ref, utsum_ref), (gtnext_ref, utnext_ref))

    def tf_take():
        for k in range(1, NZ):
            got(("tf", k), tfr.at[k])

    def fin_take(i):
        for k in range(1, NZ):
            got(("fin", i, k), finr.at[k, i])

    def write_out(i):
        tiles = ((0, 1, 2, 3), (7, 8, 9, 10), (4, 5, 6))[i]
        for q, n in enumerate(tiles):
            k = lax.rem(q + NZ - z, NZ)
            tile_out(n, finr[k, i].astype(F32))
            taps_out(n, tfr[k, i])

    def sends_done():
        for c in sent:
            c.wait_send()

    pulls[5].wait()
    pulls[6].wait()
    tf_take()
    fin_take(0)
    write_out(0)
    fin_take(1)
    write_out(1)
    eg_last()
    fin_take(2)
    write_out(2)
    sends_done()


def flush(*refs):
    sem = refs[12]
    copies = [pltpu.make_async_copy(refs[n], refs[6 + n], sem.at[n]) for n in (1, 0, 2, 3, 4, 5)]
    for c in copies:
        c.start()
    for c in copies:
        c.wait()


def per_device(
    late_rows,
    early_rows,
    hidden_cot,
    gate_weight,
    up_weight,
    gate_taps,
    up_taps,
    gate_grad_sum,
    up_grad_sum,
    gate_taps_sum,
    up_taps_sum,
):
    vmem = pl.BlockSpec(memory_space=pltpu.VMEM)
    shapes = (
        ((HALF, ROWS), BF16),
        ((ROWS, 2048), BF16),
        ((64, HALF), F32),
        ((64, HALF), F32),
        ((3, HALF), F32),
        ((3, HALF), F32),
    )
    n_sem = 240
    hbm = pl.BlockSpec(memory_space=pltpu.HBM)
    hid, *rest = pl.pallas_call(
        kernel,
        out_shape=[pltpu.VMEM(s, d) for s, d in shapes],
        in_specs=[hbm] * 11,
        out_specs=[vmem] * 6,
        scratch_shapes=[
            pltpu.VMEM((ROWS, 2048), BF16),
            pltpu.VMEM((ROWS, 2048), BF16),
            pltpu.VMEM((HALF, ROWS), BF16),
            pltpu.VMEM((64, HALF), BF16),
            pltpu.VMEM((64, HALF), BF16),
            pltpu.VMEM((64, HALF), F32),
            pltpu.VMEM((64, HALF), F32),
            pltpu.VMEM((3, HALF), BF16),
            pltpu.VMEM((3, HALF), BF16),
            pltpu.VMEM((3, HALF), F32),
            pltpu.VMEM((3, HALF), F32),
            pltpu.VMEM((64, LANE), F32),
            pltpu.VMEM((8, WIDE), F32),
            pltpu.VMEM((NY, 256, CA), BF16),
            pltpu.VMEM((NY, 256, CC), BF16),
            pltpu.VMEM((NY, 256, CB), BF16),
            pltpu.VMEM((NY, ROWS, 256), BF16),
            pltpu.VMEM((NY, ROWS, 256), BF16),
            pltpu.VMEM((NY, NZ, 256, ROWS), BF16),
            pltpu.VMEM((ROWS, WIDE), F32),
            pltpu.VMEM((ROWS, WIDE), F32),
            pltpu.VMEM((ROWS, 768), BF16),
            pltpu.VMEM((ROWS, WIDE), BF16),
            pltpu.VMEM((3, NZ, ROWS, LANE), BF16),
            pltpu.VMEM((3, NZ, ROWS, LANE), BF16),
            pltpu.VMEM((2, 3, 4, 256, LANE), BF16),
            pltpu.VMEM((2, 3, 4, 256, LANE), BF16),
            pltpu.VMEM((3, 256, LANE), BF16),
            pltpu.VMEM((NZ, 3, 64, LANE), BF16),
            pltpu.VMEM((ROWS, 2048), BF16),
            pltpu.VMEM((4, 32, 2048), BF16),
            pltpu.VMEM((4, 32, 2048), BF16),
            pltpu.VMEM((4, 32, 2048), BF16),
            pltpu.VMEM((32, 2048), BF16),
            pltpu.VMEM((NZ, 3, 8, LANE), F32),
            pltpu.VMEM((NZ, 3, 8, LANE), F32),
            pltpu.VMEM((3, 8, LANE), F32),
            pltpu.VMEM((NY, 3, 8, LANE), F32),
            pltpu.VMEM((NZ, 3, 8, LANE), F32),
            pltpu.SemaphoreType.DMA((11,)),
            pltpu.SemaphoreType.DMA((n_sem,)),
            pltpu.SemaphoreType.DMA((n_sem,)),
        ],
        compiler_params=pltpu.CompilerParams(
            collective_id=0, has_side_effects=True, vmem_limit_bytes=57000 * 1024
        ),
    )(
        late_rows,
        early_rows,
        hidden_cot.T,
        gate_weight,
        up_weight,
        gate_grad_sum,
        up_grad_sum,
        gate_taps,
        up_taps,
        gate_taps_sum,
        up_taps_sum,
    )
    hid, *rest = pl.pallas_call(
        flush,
        out_shape=[jax.ShapeDtypeStruct(s, d) for s, d in shapes],
        in_specs=[vmem] * 6,
        out_specs=[hbm] * 6,
        scratch_shapes=[pltpu.SemaphoreType.DMA((6,))],
        compiler_params=pltpu.CompilerParams(vmem_limit_bytes=8 * 1024 * 1024),
    )(hid, *rest)
    return (hid.T, *rest)


def solution(mesh):
    split = Mesh(
        mesh.devices.reshape(mesh.shape["rep"], NZ, NY, mesh.shape["tp"]),
        ("rep", "fs_0", "fs_1", "tp"),
    )
    placed = (
        P(REP_FS, None),
        P(REP_FS, None),
        P(REP_FS, "tp"),
        P(FS, "tp"),
        P(FS, "tp"),
        P(None, "tp"),
        P(None, "tp"),
        P(REP_FS, "tp"),
        P(REP_FS, "tp"),
        P("rep", "tp"),
        P("rep", "tp"),
    )
    return jax.shard_map(
        per_device,
        mesh=split,
        in_specs=placed,
        out_specs=(
            P(REP_FS, "tp"),
            P(REP_FS, None),
            P(REP_FS, "tp"),
            P(REP_FS, "tp"),
            P("rep", "tp"),
            P("rep", "tp"),
        ),
        check_vma=False,
    )
```

```python
import jax
import jax.numpy as jnp
from jax import lax
from jax.experimental import pallas as pl
from jax.experimental.pallas import tpu as pltpu
from jax.sharding import Mesh
from jax.sharding import PartitionSpec as P

FS = ("fs_0", "fs_1")
REP_FS = ("rep", "fs_0", "fs_1")
MESH = pl.DeviceIdType.MESH

NZ, NY, NT = 4, 8, 8
ROWS = 256
LANE = 128
CA, CC, CB = 512, 384, 512
AC = CA + CC
WIDE = AC + CB
HALF = 704
GPOS, UPOS = (0, 2, 4, 7, 9), (1, 3, 5, 8, 10)
F32, BF16 = jnp.float32, jnp.bfloat16
GELU_K = 0.7978845608028654
GELU_A = 0.044715


def al(v, m):
    return pl.multiple_of(v, m)


def low_lanes(shape):
    return lax.broadcasted_iota(jnp.int32, shape, 1) < 64


def swap_halves(v):
    return pltpu.roll(v, 64, 1)


def row_of(shape):
    return lax.broadcasted_iota(jnp.int32, shape, 0)


def later(v, by):
    return jnp.where(row_of(v.shape) >= by, pltpu.roll(v, by, 0), 0.0)


def sooner(v, by):
    n = v.shape[0]
    return jnp.where(row_of(v.shape) < n - by, pltpu.roll(v, n - by, 0), 0.0)


def gelu_parts(v):
    t = jnp.tanh(GELU_K * (v + GELU_A * v * v * v))
    return 0.5 * v * (1.0 + t), t


def gelu_slope(v, t):
    return 0.5 * (1.0 + t) + 0.5 * v * (1.0 - t * t) * GELU_K * (1.0 + 3.0 * GELU_A * v * v)


def kernel(
    late_hbm,
    early_hbm,
    cot_hbm,
    gw_hbm,
    uw_hbm,
    gsum_hbm,
    usum_hbm,
    gt_hbm,
    ut_hbm,
    gtsum_hbm,
    utsum_hbm,
    hid_out,
    eg_ref,
    gnext_ref,
    unext_ref,
    gtnext_ref,
    utnext_ref,
    hid_ref,
    late_ref,
    early_ref,
    cot_ref,
    gw,
    uw,
    gsum_ref,
    usum_ref,
    gt_ref,
    ut_ref,
    gtsum_ref,
    utsum_ref,
    wmix,
    taps_ref,
    wa,
    wc,
    wb,
    xe,
    xl,
    xt,
    pre,
    prel,
    cot,
    dpre,
    dpq,
    dpg,
    snd,
    rcv,
    fin,
    finr,
    dxp,
    dxc,
    dxs,
    dxr,
    egs,
    tsum,
    tzr,
    tys,
    tyr,
    tfr,
    lsem,
    ssem,
    rsem,
):
    rep = lax.axis_index("rep")
    z = lax.axis_index("fs_0")
    y = lax.axis_index("fs_1")
    t = lax.axis_index("tp")
    scale = (NZ * NY * ROWS) ** -0.5

    def ring(k):
        g = lax.rem(rep * NZ + z + 2 * NZ + k, 2 * NZ)
        return {"rep": lax.div(g, NZ), "fs_0": lax.rem(g, NZ)}

    def zdev(k):
        return {"fs_0": lax.rem(z + NZ + k, NZ)}

    def ydev(k):
        return {"fs_1": lax.rem(y + NY + k, NY)}

    def tdev(k):
        return {"tp": lax.rem(t + NT + k, NT)}

    def zat(k):
        return lax.rem(z + NZ + k, NZ)

    def yat(k):
        return lax.rem(y + NY + k, NY)

    peers = [ring(1), ring(-1), ring(2), ring(-2)]
    peers += [zdev(k) for k in range(1, NZ)]
    peers += [ydev(k) for k in range(1, NY)]
    peers += [tdev(k) for k in range(1, NT)]

    barrier = pltpu.get_barrier_semaphore()
    for dev in peers:
        pl.semaphore_signal(barrier, inc=1, device_id=dev, device_id_type=MESH)

    pulls = []
    for n, (src, dst) in enumerate(
        (
            (gw_hbm, gw),
            (uw_hbm, uw),
            (early_hbm, early_ref),
            (late_hbm, late_ref),
            (cot_hbm, cot_ref),
            (gsum_hbm, gsum_ref),
            (usum_hbm, usum_ref),
            (gt_hbm, gt_ref),
            (ut_hbm, ut_ref),
            (gtsum_hbm, gtsum_ref),
            (utsum_hbm, utsum_ref),
        )
    ):
        c = pltpu.make_async_copy(src, dst, lsem.at[n])
        c.start()
        pulls.append(c)

    arrivals, kinds = {}, {}

    def arrival(name):
        kind, rest = name[0], name[1:]
        if kind == "a1":
            rest = (rest[0], abs(rest[1]))
        elif kind == "a2":
            rest = (rest[0], rest[2], rest[3])
        elif kind == "b1":
            rest = (rest[1],)
        elif kind in ("b2", "b2f"):
            rest = (abs(rest[0]),)
        elif kind in ("xx", "xf"):
            rest = (rest[1],)
        elif kind in ("dp", "fin"):
            rest = (rest[0],)
        elif kind == "rs":
            rest = (rest[0], rest[1] % 3, rest[2])
        elif kind != "xz":
            rest = ()
        return arrivals.setdefault((kind, *rest), len(arrivals))

    def kind_of(name):
        kind = name[0]
        if kind in ("a1", "a2"):
            kind += name[1]
        elif kind in ("xz", "xx", "xf", "xc"):
            kind = "x"
        elif kind in ("dc", "dx", "eg", "ec"):
            kind = "d"
        elif kind in ("tz", "tf"):
            kind = "t"
        elif kind == "dp":
            kind = "rs"
        return kinds.setdefault(kind, len(kinds))

    def copy_of(src, dst, s, r, dev):
        return pltpu.make_async_remote_copy(
            src_ref=src,
            dst_ref=dst,
            send_sem=ssem.at[s],
            recv_sem=rsem.at[r],
            device_id=dev,
            device_id_type=MESH,
        )

    def send(name, src, dst, dev):
        copy_of(src, dst, kind_of(name), arrival(name), dev).start()

    def got(name, ref):
        copy_of(ref, ref, 0, arrival(name), ydev(1)).wait_recv()

    def gone(kind, ref):
        copy_of(ref, ref, kinds[kind], 0, ydev(1)).wait_send()

    def wrow(zz, first, n):
        return pl.ds(al(zz * 64 + first, 32), n)

    own = wrow(z, 0, 64)

    pulls[0].wait()
    pulls[1].wait()
    wmix[:, 0:64] = gw[:, 640:HALF].astype(F32)
    wmix[:, 64:LANE] = uw[:, 640:HALF].astype(F32)
    wc[y, own, 256:CC] = wmix[...].astype(BF16)
    for n in range(5):
        cols = slice(n * LANE, (n + 1) * LANE)
        for src, pos in ((gw, GPOS[n]), (uw, UPOS[n])):
            here = slice(pos * LANE, (pos + 1) * LANE)
            if pos < 4:
                wa[y, own, here] = src[:, cols]
            elif pos < 7:
                wc[y, own, (pos - 4) * LANE : (pos - 3) * LANE] = src[:, cols]
            else:
                wb[y, own, (pos - 7) * LANE : (pos - 6) * LANE] = src[:, cols]
    pl.semaphore_wait(barrier, len(peers))

    def zrow(q):
        return zat((0, -1, 1, 2)[q])

    wide = {"a": wa, "c": wc}

    def a2_own(p, q):
        blk = wide[p].at[y, wrow(zrow(q), 0, 64)]
        for d in (1, -1):
            send(("a2", p, d, 0, q), blk, blk, ydev(d))

    def a1_send(p, near):
        if near:
            blk = wide[p].at[y, own]
            for k in (1, -1):
                send(("a1", p, k), blk, blk, ring(k))
            return
        for h, k in ((0, 2), (1, -2)):
            blk = wide[p].at[y, wrow(z, 32 * h, 32)]
            send(("a1", p, k), blk, blk, ring(k))

    b_own = wb.at[y, own]
    a1_send("a", True)
    for h, d in ((0, 1), (1, -1), (1, 1), (0, -1)):
        blk = wb.at[y, wrow(z, 32 * h, 32)]
        send(("b1", d, 0, h), blk, blk, ydev(d))
    a1_send("a", False)
    a2_own("a", 0)
    for k in (1, -1):
        send(("b2", 0, k), b_own, b_own, ring(k))
    a1_send("c", True)
    a1_send("c", False)

    def order_rows(src_ref, dst):
        def one(yp, carry):
            for zp in range(2):
                a = src_ref[:, pl.ds(al(2 * zp * 512 + yp * LANE, LANE), LANE)].astype(F32)
                b = src_ref[:, pl.ds(al((2 * zp + 1) * 512 + yp * LANE, LANE), LANE)].astype(F32)
                low = low_lanes(a.shape)
                cols = slice(zp * LANE, (zp + 1) * LANE)
                dst[2 * yp, :, cols] = jnp.where(low, a, swap_halves(b)).astype(BF16)
                dst[2 * yp + 1, :, cols] = jnp.where(low, swap_halves(a), b).astype(BF16)
            return carry

        lax.fori_loop(0, NY // 2, one, 0)

    pulls[2].wait()
    order_rows(early_ref, xe)

    def turn(yb, carry):
        xt[yb, 0] = xe[yb].astype(F32).T.astype(BF16)
        return carry

    lax.fori_loop(0, NY, turn, 0)

    def x_send(k):
        send(("xz", k), xt.at[t, 0], xt.at[t, k], zdev(-k))

    pair = {"tp": t + 1 - 2 * lax.rem(t, 2)}

    def x_take(j):
        blk = xt.at[t, j]
        got(("xz", j), blk)
        for k in (2, 6):
            send(("xx", k, j), blk, blk, tdev(k))
        send(("xc", 0, j), blk, blk, pair)

    def x_mid(j):
        got(("xx", 2, j), xt.at[0, pl.ds(0, 2)])
        for k, h in ((2, 0), (6, 128)):
            row = lax.rem(t + NT - k, NT)
            blk = xt.at[row, j]
            half = xt.at[row, j, pl.ds(h, 128)]
            send(("xf", k, j), half, half, tdev(k))
            send(("xc", k, j), blk, blk, pair)

    def x_far(j):
        row = lax.rem(t + 4, NT)
        blk = xt.at[row, j]
        got(("xf", 2, j), blk)
        send(("xc", 4, j), blk, blk, pair)

    def x_last():
        got(("xc", 0, 1), xt.at[pl.ds(0, 4), pl.ds(0, 3)])

    def a1_near(p):
        got(("a1", p, 1), wide[p].at[0, pl.ds(0, 128)])

    def a1_far(p):
        got(("a1", p, 2), wide[p].at[0, pl.ds(0, 64)])

    def a2_last(d):
        return (0, 1) if d == 1 else (2, 3)

    def a2_take(p, s, qs):
        for q in qs:
            got(("a2", p, 1, s - 1, q), wide[p].at[0, pl.ds(0, 64 if s == 4 else 128)])
            for d in (1, -1):
                blk = wide[p].at[yat(-d * s), wrow(zrow(q), 0, 64)]
                if s < 3 or (s == 3 and q in a2_last(d)):
                    send(("a2", p, d, s, q), blk, blk, ydev(d))

    def b1_take(s):
        got(("b1", 1, s - 1, 0), wb.at[0, pl.ds(0, 64 if s == 4 else 128)])
        for d in (1, -1):
            mine = 0 if d == 1 else 1
            for h in (mine, 1 - mine):
                blk = wb.at[yat(-d * s), wrow(z, 32 * h, 32)]
                if s < 3 or (s == 3 and h == mine):
                    send(("b1", d, s, h), blk, blk, ydev(d))
        for e in ordinals(s):
            blk = wb.at[yat(-e), own]
            for k in (1, -1):
                send(("b2", e, k), blk, blk, ring(k))

    def ordinals(s):
        return (0,) if s == 0 else ((4,) if s == 4 else (s, -s))

    def b2_take(s):
        got(("b2", s, 1), wb.at[0, pl.ds(0, 128 * len(ordinals(s)))])
        for e in ordinals(s):
            for k in (1, -1):
                yb = yat(-e)
                half = wb.at[yb, wrow(zat(-k), 0 if k == 1 else 32, 32)]
                send(("b2f", e, k), half, half, ring(k))

    def b2f_take(s):
        got(("b2f", s, 1), wb.at[0, pl.ds(0, 64 * len(ordinals(s)))])

    def project(w, first, width, yb, start):
        rows = xe[yb]

        def tile(c0, n):
            cols = pl.ds(first + c0, n)
            part = jnp.dot(rows, w[yb, :, pl.ds(c0, n)], preferred_element_type=F32)
            pre[:, cols] = part if start else pre[:, cols] + part

        def one(c, carry):
            tile(al(c * 256, 256), 256)
            return carry

        lax.fori_loop(0, width // 256, one, 0)
        if width % 256:
            tile(width - width % 256, width % 256)

    def late_project(w, first, c0, n):
        v = jnp.dot(xl[0], w[0, :, c0 : c0 + n], preferred_element_type=F32)
        for yb in range(1, NY):
            v = v + jnp.dot(xl[yb], w[yb, :, c0 : c0 + n], preferred_element_type=F32)
        prel[:, first + c0 : first + c0 + n] = v

    def project_a(s):
        for e in ordinals(s):
            project(wa, 0, CA, yat(-e), s == 0)

    def project_c(s):
        for e in ordinals(s):
            project(wc, CA, CC, yat(-e), s == 0)

    def project_b(s):
        for e in ordinals(s):
            project(wb, AC, CB, yat(-e), s == 0)

    def join_taps():
        for n in range(7, 11):
            pulls[n].wait()
        for n in range(5):
            cols = slice(n * LANE, (n + 1) * LANE)
            for src, pos in ((gt_ref, GPOS[n]), (ut_ref, UPOS[n])):
                taps_ref[0:3, pos * LANE : (pos + 1) * LANE] = src[:, cols].astype(F32)
        taps_ref[0:3, 768:832] = gt_ref[:, 640:HALF].astype(F32)
        taps_ref[0:3, 832:AC] = ut_ref[:, 640:HALF].astype(F32)

    def turn_cot():
        for n in range(5):
            v = cot_ref[n * LANE : (n + 1) * LANE, :].astype(F32).T
            cot[:, n * LANE : (n + 1) * LANE] = v.astype(BF16)
        cot[:, 640:768] = jnp.zeros((ROWS, LANE), BF16)
        cot[:, 640:HALF] = cot_ref[640:HALF, :].astype(F32).T.astype(BF16)

    def tap(cols):
        return [taps_ref[j : j + 1, cols] for j in range(3)]

    def mixed(src, cols):
        v = src[:, cols].astype(BF16).astype(F32)
        w = tap(cols)
        return v, w[0] * later(v, 2) + w[1] * later(v, 1) + w[2] * v, w

    def back(d, v, w, cols, i, q):
        r = (w[2] * d + w[1] * sooner(d, 1) + w[0] * sooner(d, 2)).astype(BF16)
        dpre[:, cols] = r
        dpq[i, q] = r
        for j, u in enumerate((later(v, 2), later(v, 1), v)):
            tsum[q, i, j : j + 1, :] = jnp.sum(d * u, axis=0, keepdims=True) * scale

    def tile_cols(n):
        return pl.ds(al(n * LANE, LANE), LANE)

    tsum[...] = jnp.zeros_like(tsum)
    dpq[2, 3] = jnp.zeros((ROWS, LANE), BF16)

    def early_pair(n, gpos, upos, i, q):
        gc, uc = tile_cols(gpos), tile_cols(upos)
        gv, gm, gw_ = mixed(pre, gc)
        uv, um, uw_ = mixed(pre, uc)
        c = cot[:, tile_cols(n)].astype(F32)
        act, th = gelu_parts(gm)
        back(c * um * gelu_slope(gm, th), gv, gw_, gc, i, q)
        back(c * act, uv, uw_, uc, i, q + 1)

    def early_a(n, carry):
        early_pair(n, 2 * n, 2 * n + 1, 0, 2 * n)
        return carry

    def early_b(m, carry):
        early_pair(m + 3, 2 * m + 7, 2 * m + 8, 1, 2 * m)
        return carry

    last = slice(768, AC)

    def early_c():
        early_pair(2, 4, 5, 2, 0)
        mv, mm, mw = mixed(pre, last)
        c = cot[:, 640:768].astype(F32)
        act, th = gelu_parts(mm)
        dg = c * swap_halves(mm) * gelu_slope(mm, th)
        du = swap_halves(c * act)
        back(jnp.where(low_lanes(dg.shape), dg, du), mv, mw, last, 2, 2)
        for k in range(1, NZ):
            send(("tz", k), tsum.at[zat(-k)], tzr.at[k], zdev(-k))

    def dp_send(i):
        for k in range(1, NZ):
            send(("dp", i, k), dpq.at[i, zat(-k)], dpg.at[i, k], zdev(-k))
        dpg[i, 0] = dpq[i, z]

    def dx(yb, carry):
        nt = (((1,), (1,)), ((), ()))
        v = lax.dot_general(dpre[:, 0:CA], wa[yb], nt, preferred_element_type=F32)
        v = v + lax.dot_general(dpre[:, CA:AC], wc[yb], nt, preferred_element_type=F32)
        v = v + lax.dot_general(dpre[:, AC:WIDE], wb[yb], nt, preferred_element_type=F32)
        dxp[:, pl.ds(al(yb * 256, 256), 256)] = v.astype(BF16)
        return carry

    def strip(tt):
        return pl.ds(al(tt * 32, 32), 32)

    core = lax.rem(t, 2)

    def dx_send():
        for x in range(4):
            send(("dc", x), dxp.at[strip(2 * x + 1 - core)], dxc.at[x], pair)

    def dx_pair():
        got(("dc", 0), dxc)
        for x in range(4):
            v = dxp[strip(2 * x + core), :].astype(F32) + dxc[x].astype(F32)
            dxs[x] = v.astype(BF16)
        for k in (2, 6, 4):
            to = lax.div(lax.rem(t + NT - k, NT), 2)
            send(("dx", k), dxs.at[to], dxr.at[k // 2], tdev(-k))

    def taps_first():
        got(("tz", 1), tzr.at[pl.ds(1, 3)])
        tys[...] = tsum[z] + tzr[1] + tzr[2] + tzr[3]
        for k in range(1, NY):
            send(("ty", k), tys, tyr.at[k], ydev(-k))

    def term(i, yb):
        v = jnp.dot(xt[yb, 0], dpg[i, 0], preferred_element_type=F32)
        for k in range(1, NZ):
            v = v + jnp.dot(xt[yb, k], dpg[i, k], preferred_element_type=F32)
        return v * scale

    def side(d):
        return 0 if d == 1 else 1

    def part(d):
        return pl.ds(0, 128) if d == 1 else pl.ds(128, 128)

    def rs(i, s):
        if s == 0:
            got(("dp", i, 1), dpg.at[i, pl.ds(1, 3)])
            for d in (1, -1):
                buf = snd.at[side(d), i, 0]
                buf[...] = term(i, yat(3 * d)).astype(BF16)
                send(("rs", i, 0, d), buf, rcv.at[side(d), i, 0], ydev(d))
            v = term(i, yat(4))
            for d in (1, -1):
                buf = snd.at[side(d), i, 3, part(d)]
                buf[...] = (v[0:128] if d == 1 else v[128:256]).astype(BF16)
                send(("rs", i, 3, d), buf, rcv.at[side(d), i, 3, part(d)], ydev(2 * d))
            return
        if s < 3:
            for d in (1, -1):
                v = term(i, yat(d * (3 - s)))
                if s == 1:
                    got(("rs", i, 0, d), xt.at[0, 0, pl.ds(0, 192)])
                else:
                    got(("rs", i, s - 1, d), rcv.at[side(d), i, s - 1])
                v = v + rcv[side(d), i, s - 1].astype(F32)
                buf = snd.at[side(d), i, s]
                if s == 1:
                    w = rcv[side(d), i, 3, part(d), :].astype(F32)
                    if d == 1:
                        buf[0:128, :] = (v[0:128] + w).astype(BF16)
                        buf[128:256, :] = v[128:256].astype(BF16)
                    else:
                        buf[0:128, :] = v[0:128].astype(BF16)
                        buf[128:256, :] = (v[128:256] + w).astype(BF16)
                else:
                    buf[...] = v.astype(BF16)
                send(("rs", i, s, d), buf, rcv.at[side(d), i, s], ydev(d))
            return
        v = term(i, y)
        for d in (1, -1):
            got(("rs", i, 2, d), rcv.at[side(d), i, 2])
            v = v + rcv[side(d), i, 2].astype(F32)
        fin[i] = v.astype(BF16)
        for k in range(1, NZ):
            send(("fin", i, k), fin.at[i, wrow(zat(-k), 0, 64)], finr.at[k, i], zdev(-k))
        finr[0, i] = fin[i, own, :]

    def eg_own():
        return pltpu.make_async_copy(egs, eg_ref.at[strip(t)], lsem.at[11])

    def hid_flush():
        return pltpu.make_async_copy(hid_ref, hid_out, lsem.at[12])

    def dx_reduce():
        v = dxs[lax.div(t, 2)].astype(F32)
        got(("dx", 2), dxr.at[pl.ds(1, 3)])
        for k in (2, 6, 4):
            v = v + dxr[k // 2].astype(F32)
        for yp in range(NY // 2):
            for zp in range(2):
                a = v[:, 2 * yp * 256 + zp * LANE : 2 * yp * 256 + (zp + 1) * LANE]
                b = v[:, (2 * yp + 1) * 256 + zp * LANE : (2 * yp + 1) * 256 + (zp + 1) * LANE]
                low = low_lanes(a.shape)
                at0 = 2 * zp * 512 + yp * LANE
                egs[:, at0 : at0 + LANE] = jnp.where(low, a, swap_halves(b)).astype(BF16)
                egs[:, at0 + 512 : at0 + 512 + LANE] = jnp.where(low, swap_halves(a), b).astype(BF16)
        for k in (2, 6, 4):
            send(("eg", k), egs, eg_ref.at[strip(t)], tdev(k))
        send(("ec", 0), egs, eg_ref.at[strip(t)], pair)
        eg_own().start()

    def eg_cross():
        got(("eg", 2), dxr.at[pl.ds(1, 3)])
        for k in (2, 6, 4):
            here = eg_ref.at[strip(lax.rem(t + NT - k, NT))]
            send(("ec", k), here, here, pair)

    def eg_last():
        got(("ec", 0), dxc)

    def taps_finish():
        v = tys[...]
        got(("ty", 1), tyr.at[pl.ds(1, 7)])
        for k in range(1, NY):
            v = v + tyr[k]
        tfr[0] = v
        for k in range(1, NZ):
            send(("tf", k), tfr.at[0], tfr.at[k], zdev(-k))

    def late_pair(n, gpos, upos):
        _, gm, _ = mixed(prel, tile_cols(gpos))
        _, um, _ = mixed(prel, tile_cols(upos))
        act, _ = gelu_parts(gm)
        hid_ref[tile_cols(n), :] = (act * um).T.astype(BF16)

    def late_a(n, carry):
        late_pair(n, 2 * n, 2 * n + 1)
        return carry

    def late_b(m, carry):
        late_pair(m + 3, 2 * m + 7, 2 * m + 8)
        return carry

    def late_c():
        late_pair(2, 4, 5)
        _, mm, _ = mixed(prel, last)
        act, _ = gelu_parts(mm)
        hid_ref[640:HALF, :] = (act * swap_halves(mm)).T[0:64].astype(BF16)

    b1_take(1)
    a1_near("a")
    a2_own("a", 1)
    a2_own("a", 2)
    a2_take("a", 1, (0,))
    a1_far("a")
    a2_own("a", 3)
    b2_take(0)
    x_send(1)
    a2_take("a", 1, (1,))
    b1_take(2)
    x_send(2)
    a2_take("a", 1, (2,))
    a2_take("a", 1, (3,))
    b2_take(1)
    x_send(3)
    pulls[3].wait()
    order_rows(late_ref, xl)
    b1_take(3)
    a2_take("a", 2, (0, 1))
    project_a(0)
    a2_take("a", 2, (2, 3))
    b2_take(2)
    b1_take(4)
    x_take(1)
    a1_near("c")
    a1_far("c")
    a2_take("a", 3, (0,))
    a2_own("c", 0)
    project_a(1)
    a2_take("a", 3, (1,))
    a2_own("c", 1)
    a2_take("a", 3, (2,))
    a2_own("c", 2)
    a2_take("a", 3, (3,))
    a2_own("c", 3)
    x_take(2)
    project_a(2)
    b2_take(3)
    x_take(3)
    a2_take("a", 4, range(NZ))
    a2_take("c", 1, (0,))
    x_mid(1)
    project_a(3)
    a2_take("c", 1, (1,))
    b2_take(4)
    project_a(4)
    a2_take("c", 1, (2,))
    x_mid(2)
    pulls[4].wait()
    turn_cot()
    join_taps()
    lax.fori_loop(0, 2, early_a, 0)
    dp_send(0)
    a2_take("c", 1, (3,))
    b2f_take(0)
    project_b(0)
    x_far(1)
    b2f_take(1)
    project_b(1)
    a2_take("c", 2, (0, 1))
    x_mid(3)
    b2f_take(2)
    project_b(2)
    a2_take("c", 2, (2,))
    x_far(2)
    a2_take("c", 2, (3,))
    b2f_take(3)
    project_b(3)
    b2f_take(4)
    project_b(4)
    a2_take("c", 3, (0,))
    lax.fori_loop(0, 2, early_b, 0)
    dp_send(1)
    a2_take("c", 3, (1,))
    x_far(3)
    project_c(0)
    a2_take("c", 3, (2, 3))
    project_c(1)
    project_c(2)
    project_c(3)
    x_last()
    rs(0, 0)
    a2_take("c", 4, range(NZ))
    project_c(4)
    early_c()
    dp_send(2)
    lax.fori_loop(0, NY, dx, 0)
    dx_send()
    rs(1, 0)
    rs(0, 1)
    dx_pair()
    taps_first()
    rs(2, 0)
    rs(0, 2)
    rs(1, 1)
    late_project(wa, 0, 0, 256)
    late_project(wa, 0, 256, 256)
    rs(2, 1)
    rs(0, 3)
    rs(1, 2)
    late_project(wc, CA, 0, 256)
    dx_reduce()
    rs(2, 2)
    rs(1, 3)
    late_project(wc, CA, 256, 128)
    late_project(wb, AC, 0, 256)
    late_project(wb, AC, 256, 256)
    taps_finish()
    eg_cross()
    lax.fori_loop(0, 2, late_a, 0)
    rs(2, 3)
    lax.fori_loop(0, 2, late_b, 0)
    late_c()
    hid_flush().start()

    def spread(pos, v, prev, nxt):
        (gs, us), (gn, un) = prev, nxt
        if pos == 6:
            gn[:, 640:HALF] = gs[:, 640:HALF] + v[:, 0:64]
            un[:, 640:HALF] = us[:, 640:HALF] + swap_halves(v)[:, 0:64]
            return
        side_, n = (0, GPOS.index(pos)) if pos in GPOS else (1, UPOS.index(pos))
        cols = slice(n * LANE, (n + 1) * LANE)
        nxt[side_][:, cols] = prev[side_][:, cols] + v

    def tile_out(pos, v):
        spread(pos, v, (gsum_ref, usum_ref), (gnext_ref, unext_ref))

    def taps_out(pos, v):
        if pos == 6:
            gtnext_ref[:, 640:HALF] = gtsum_ref[:, 640:HALF] + v[0:3, 0:64]
            utnext_ref[:, 640:HALF] = utsum_ref[:, 640:HALF] + swap_halves(v)[0:3, 0:64]
            return
        spread(pos, v[0:3], (gtsum_ref, utsum_ref), (gtnext_ref, utnext_ref))

    def tf_take():
        got(("tf", 1), tfr.at[pl.ds(1, 3)])

    def fin_take(i):
        got(("fin", i, 1), finr.at[pl.ds(1, 3), i])

    def write_out(i):
        tiles = ((0, 1, 2, 3), (7, 8, 9, 10), (4, 5, 6))[i]
        for q, n in enumerate(tiles):
            k = lax.rem(q + NZ - z, NZ)
            tile_out(n, finr[k, i].astype(F32))
            taps_out(n, tfr[k, i])

    def sends_done():
        eg_own().wait()
        hid_flush().wait()
        gone("a1a", wa.at[0, pl.ds(0, 192)])
        gone("a1c", wc.at[0, pl.ds(0, 192)])
        gone("a2a", wa.at[pl.ds(0, 7)])
        gone("a2c", wc.at[pl.ds(0, 7)])
        gone("b1", wb.at[pl.ds(0, 7), pl.ds(0, 64)])
        gone("b2", wb.at[pl.ds(0, 4)])
        gone("b2f", wb.at[pl.ds(0, 2)])
        gone("x", xt.at[pl.ds(0, 6)])
        gone("rs", xt.at[pl.ds(0, 5), pl.ds(0, 3)])
        gone("fin", finr.at[pl.ds(0, 3)])
        gone("t", tyr.at[pl.ds(0, 6)])
        gone("ty", tyr.at[pl.ds(0, 7)])
        gone("d", xt.at[pl.ds(0, 7), pl.ds(0, 2)])

    pulls[5].wait()
    pulls[6].wait()
    tf_take()
    fin_take(0)
    write_out(0)
    fin_take(1)
    write_out(1)
    eg_last()
    fin_take(2)
    write_out(2)
    sends_done()


def flush(*refs):
    sem = refs[12]
    copies = [pltpu.make_async_copy(refs[n], refs[6 + n], sem.at[n]) for n in (1, 0, 2, 3, 4, 5)]
    for c in copies:
        c.start()
    for c in copies:
        c.wait()


def per_device(
    late_rows,
    early_rows,
    hidden_cot,
    gate_weight,
    up_weight,
    gate_taps,
    up_taps,
    gate_grad_sum,
    up_grad_sum,
    gate_taps_sum,
    up_taps_sum,
):
    vmem = pl.BlockSpec(memory_space=pltpu.VMEM)
    shapes = (
        ((HALF, ROWS), BF16),
        ((ROWS, 2048), BF16),
        ((64, HALF), F32),
        ((64, HALF), F32),
        ((3, HALF), F32),
        ((3, HALF), F32),
    )
    n_sem = 91
    hbm = pl.BlockSpec(memory_space=pltpu.HBM)
    hid, *rest = pl.pallas_call(
        kernel,
        out_shape=[pltpu.VMEM(s, d) for s, d in shapes],
        in_specs=[hbm] * 11,
        out_specs=[pl.BlockSpec(memory_space=pl.ANY)] * 2 + [vmem] * 4,
        scratch_shapes=[
            pltpu.VMEM((HALF, ROWS), BF16),
            pltpu.VMEM((ROWS, 2048), BF16),
            pltpu.VMEM((ROWS, 2048), BF16),
            pltpu.VMEM((HALF, ROWS), BF16),
            pltpu.VMEM((64, HALF), BF16),
            pltpu.VMEM((64, HALF), BF16),
            pltpu.VMEM((64, HALF), F32),
            pltpu.VMEM((64, HALF), F32),
            pltpu.VMEM((3, HALF), BF16),
            pltpu.VMEM((3, HALF), BF16),
            pltpu.VMEM((3, HALF), F32),
            pltpu.VMEM((3, HALF), F32),
            pltpu.VMEM((64, LANE), F32),
            pltpu.VMEM((8, WIDE), F32),
            pltpu.VMEM((NY, 256, CA), BF16),
            pltpu.VMEM((NY, 256, CC), BF16),
            pltpu.VMEM((NY, 256, CB), BF16),
            pltpu.VMEM((NY, ROWS, 256), BF16),
            pltpu.VMEM((NY, ROWS, 256), BF16),
            pltpu.VMEM((NY, NZ, 256, ROWS), BF16),
            pltpu.VMEM((ROWS, WIDE), F32),
            pltpu.VMEM((ROWS, WIDE), F32),
            pltpu.VMEM((ROWS, 768), BF16),
            pltpu.VMEM((ROWS, WIDE), BF16),
            pltpu.VMEM((3, NZ, ROWS, LANE), BF16),
            pltpu.VMEM((3, NZ, ROWS, LANE), BF16),
            pltpu.VMEM((2, 3, 4, 256, LANE), BF16),
            pltpu.VMEM((2, 3, 4, 256, LANE), BF16),
            pltpu.VMEM((3, 256, LANE), BF16),
            pltpu.VMEM((NZ, 3, 64, LANE), BF16),
            pltpu.VMEM((ROWS, 2048), BF16),
            pltpu.VMEM((4, 32, 2048), BF16),
            pltpu.VMEM((4, 32, 2048), BF16),
            pltpu.VMEM((4, 32, 2048), BF16),
            pltpu.VMEM((32, 2048), BF16),
            pltpu.VMEM((NZ, 3, 8, LANE), F32),
            pltpu.VMEM((NZ, 3, 8, LANE), F32),
            pltpu.VMEM((3, 8, LANE), F32),
            pltpu.VMEM((NY, 3, 8, LANE), F32),
            pltpu.VMEM((NZ, 3, 8, LANE), F32),
            pltpu.SemaphoreType.DMA((13,)),
            pltpu.SemaphoreType.DMA((13,)),
            pltpu.SemaphoreType.DMA((n_sem,)),
        ],
        compiler_params=pltpu.CompilerParams(
            collective_id=0, has_side_effects=True, vmem_limit_bytes=57000 * 1024
        ),
    )(
        late_rows,
        early_rows,
        hidden_cot.T,
        gate_weight,
        up_weight,
        gate_grad_sum,
        up_grad_sum,
        gate_taps,
        up_taps,
        gate_taps_sum,
        up_taps_sum,
    )
    hid, *rest = pl.pallas_call(
        flush,
        out_shape=[jax.ShapeDtypeStruct(s, d) for s, d in shapes],
        in_specs=[vmem] * 6,
        out_specs=[hbm] * 6,
        scratch_shapes=[pltpu.SemaphoreType.DMA((6,))],
        compiler_params=pltpu.CompilerParams(vmem_limit_bytes=8 * 1024 * 1024),
    )(hid, *rest)
    return (hid.T, *rest)


def solution(mesh):
    split = Mesh(
        mesh.devices.reshape(mesh.shape["rep"], NZ, NY, mesh.shape["tp"]),
        ("rep", "fs_0", "fs_1", "tp"),
    )
    placed = (
        P(REP_FS, None),
        P(REP_FS, None),
        P(REP_FS, "tp"),
        P(FS, "tp"),
        P(FS, "tp"),
        P(None, "tp"),
        P(None, "tp"),
        P(REP_FS, "tp"),
        P(REP_FS, "tp"),
        P("rep", "tp"),
        P("rep", "tp"),
    )
    return jax.shard_map(
        per_device,
        mesh=split,
        in_specs=placed,
        out_specs=(
            P(REP_FS, "tp"),
            P(REP_FS, None),
            P(REP_FS, "tp"),
            P(REP_FS, "tp"),
            P("rep", "tp"),
            P("rep", "tp"),
        ),
        check_vma=False,
    )
```

```python
import jax
import jax.numpy as jnp
from jax import lax
from jax.experimental import pallas as pl
from jax.experimental.pallas import tpu as pltpu
from jax.sharding import Mesh
from jax.sharding import PartitionSpec as P

FS = ("fs_0", "fs_1")
REP_FS = ("rep", "fs_0", "fs_1")
MESH = pl.DeviceIdType.MESH

NZ, NY, NT = 4, 8, 8
ROWS = 256
LANE = 128
CA, CC, CB = 512, 384, 512
AC = CA + CC
WIDE = AC + CB
HALF = 704
GPOS, UPOS = (0, 2, 4, 7, 9), (1, 3, 5, 8, 10)
F32, BF16 = jnp.float32, jnp.bfloat16
GELU_K = 0.7978845608028654
GELU_A = 0.044715


def al(v, m):
    return pl.multiple_of(v, m)


def low_lanes(shape):
    return lax.broadcasted_iota(jnp.int32, shape, 1) < 64


def swap_halves(v):
    return pltpu.roll(v, 64, 1)


def row_of(shape):
    return lax.broadcasted_iota(jnp.int32, shape, 0)


def later(v, by):
    return jnp.where(row_of(v.shape) >= by, pltpu.roll(v, by, 0), 0.0)


def sooner(v, by):
    n = v.shape[0]
    return jnp.where(row_of(v.shape) < n - by, pltpu.roll(v, n - by, 0), 0.0)


def gelu_parts(v):
    t = jnp.tanh(GELU_K * (v + GELU_A * v * v * v))
    return 0.5 * v * (1.0 + t), t


def gelu_slope(v, t):
    return 0.5 * (1.0 + t) + 0.5 * v * (1.0 - t * t) * GELU_K * (1.0 + 3.0 * GELU_A * v * v)


def kernel(
    late_hbm,
    early_hbm,
    cot_hbm,
    gw_hbm,
    uw_hbm,
    gsum_hbm,
    usum_hbm,
    gt_hbm,
    ut_hbm,
    gtsum_hbm,
    utsum_hbm,
    hid_out,
    eg_ref,
    gnext_ref,
    unext_ref,
    gtnext_ref,
    utnext_ref,
    hid_ref,
    late_ref,
    early_ref,
    cot_ref,
    gw,
    uw,
    gsum_ref,
    usum_ref,
    gt_ref,
    ut_ref,
    gtsum_ref,
    utsum_ref,
    wmix,
    taps_ref,
    wa,
    wc,
    wb,
    xe,
    xl,
    xt,
    pre,
    prel,
    cot,
    dpre,
    dpq,
    dpg,
    snd,
    rcv,
    fin,
    finr,
    dxp,
    dxc,
    dxs,
    dxr,
    egs,
    tsum,
    tzr,
    tys,
    tyr,
    tfr,
    lsem,
    ssem,
    rsem,
):
    rep = lax.axis_index("rep")
    z = lax.axis_index("fs_0")
    y = lax.axis_index("fs_1")
    t = lax.axis_index("tp")
    scale = (NZ * NY * ROWS) ** -0.5

    def ring(k):
        g = lax.rem(rep * NZ + z + 2 * NZ + k, 2 * NZ)
        return {"rep": lax.div(g, NZ), "fs_0": lax.rem(g, NZ)}

    def zdev(k):
        return {"fs_0": lax.rem(z + NZ + k, NZ)}

    def ydev(k):
        return {"fs_1": lax.rem(y + NY + k, NY)}

    def tdev(k):
        return {"tp": lax.rem(t + NT + k, NT)}

    def zat(k):
        return lax.rem(z + NZ + k, NZ)

    def yat(k):
        return lax.rem(y + NY + k, NY)

    peers = [ring(1), ring(-1), ring(2), ring(-2)]
    peers += [zdev(k) for k in range(1, NZ)]
    peers += [ydev(k) for k in range(1, NY)]
    peers += [tdev(k) for k in range(1, NT)]

    barrier = pltpu.get_barrier_semaphore()
    for dev in peers:
        pl.semaphore_signal(barrier, inc=1, device_id=dev, device_id_type=MESH)

    pulls = []
    for n, (src, dst) in enumerate(
        (
            (gw_hbm, gw),
            (uw_hbm, uw),
            (early_hbm, early_ref),
            (late_hbm, late_ref),
            (cot_hbm, cot_ref),
            (gsum_hbm, gsum_ref),
            (usum_hbm, usum_ref),
            (gt_hbm, gt_ref),
            (ut_hbm, ut_ref),
            (gtsum_hbm, gtsum_ref),
            (utsum_hbm, utsum_ref),
        )
    ):
        c = pltpu.make_async_copy(src, dst, lsem.at[n])
        c.start()
        pulls.append(c)

    arrivals, kinds = {}, {}

    def arrival(name):
        kind, rest = name[0], name[1:]
        if kind == "a1":
            rest = (rest[0], abs(rest[1]))
        elif kind == "a2":
            rest = (rest[0], rest[2], rest[3])
        elif kind == "b1":
            rest = (rest[1],)
        elif kind in ("b2", "b2f"):
            rest = (abs(rest[0]),)
        elif kind in ("xx", "xf"):
            rest = (rest[1],)
        elif kind in ("dp", "fin"):
            rest = (rest[0],)
        elif kind == "rs":
            rest = (rest[0], rest[1] % 3, rest[2])
        elif kind != "xz":
            rest = ()
        return arrivals.setdefault((kind, *rest), len(arrivals))

    def kind_of(name):
        kind = name[0]
        if kind in ("a1", "a2"):
            kind += name[1]
        elif kind in ("xz", "xx", "xf", "xc"):
            kind = "x"
        elif kind in ("dc", "dx", "eg", "ec"):
            kind = "d"
        elif kind in ("tz", "tf"):
            kind = "t"
        elif kind == "dp":
            kind = "rs"
        return kinds.setdefault(kind, len(kinds))

    def copy_of(src, dst, s, r, dev):
        return pltpu.make_async_remote_copy(
            src_ref=src,
            dst_ref=dst,
            send_sem=ssem.at[s],
            recv_sem=rsem.at[r],
            device_id=dev,
            device_id_type=MESH,
        )

    def send(name, src, dst, dev):
        copy_of(src, dst, kind_of(name), arrival(name), dev).start()

    def got(name, ref):
        copy_of(ref, ref, 0, arrival(name), ydev(1)).wait_recv()

    def gone(kind, ref):
        copy_of(ref, ref, kinds[kind], 0, ydev(1)).wait_send()

    def wrow(zz, first, n):
        return pl.ds(al(zz * 64 + first, 32), n)

    own = wrow(z, 0, 64)

    pulls[0].wait()
    pulls[1].wait()
    wmix[:, 0:64] = gw[:, 640:HALF].astype(F32)
    wmix[:, 64:LANE] = uw[:, 640:HALF].astype(F32)
    wc[y, own, 256:CC] = wmix[...].astype(BF16)
    for n in range(5):
        cols = slice(n * LANE, (n + 1) * LANE)
        for src, pos in ((gw, GPOS[n]), (uw, UPOS[n])):
            here = slice(pos * LANE, (pos + 1) * LANE)
            if pos < 4:
                wa[y, own, here] = src[:, cols]
            elif pos < 7:
                wc[y, own, (pos - 4) * LANE : (pos - 3) * LANE] = src[:, cols]
            else:
                wb[y, own, (pos - 7) * LANE : (pos - 6) * LANE] = src[:, cols]
    pl.semaphore_wait(barrier, len(peers))

    def zrow(q):
        return zat((0, -1, 1, 2)[q])

    wide = {"a": wa, "c": wc}

    def a2_own(p, q):
        blk = wide[p].at[y, wrow(zrow(q), 0, 64)]
        for d in (1, -1):
            send(("a2", p, d, 0, q), blk, blk, ydev(d))

    def a1_send(p, near):
        if near:
            blk = wide[p].at[y, own]
            for k in (1, -1):
                send(("a1", p, k), blk, blk, ring(k))
            return
        for h, k in ((0, 2), (1, -2)):
            blk = wide[p].at[y, wrow(z, 32 * h, 32)]
            send(("a1", p, k), blk, blk, ring(k))

    b_own = wb.at[y, own]
    a1_send("a", True)
    for h, d in ((0, 1), (1, -1), (1, 1), (0, -1)):
        blk = wb.at[y, wrow(z, 32 * h, 32)]
        send(("b1", d, 0, h), blk, blk, ydev(d))
    a1_send("a", False)
    a2_own("a", 0)
    for k in (1, -1):
        send(("b2", 0, k), b_own, b_own, ring(k))
    a1_send("c", True)
    a1_send("c", False)

    def order_rows(src_ref, dst):
        def one(yp, carry):
            for zp in range(2):
                a = src_ref[:, pl.ds(al(2 * zp * 512 + yp * LANE, LANE), LANE)].astype(F32)
                b = src_ref[:, pl.ds(al((2 * zp + 1) * 512 + yp * LANE, LANE), LANE)].astype(F32)
                low = low_lanes(a.shape)
                cols = slice(zp * LANE, (zp + 1) * LANE)
                dst[2 * yp, :, cols] = jnp.where(low, a, swap_halves(b)).astype(BF16)
                dst[2 * yp + 1, :, cols] = jnp.where(low, swap_halves(a), b).astype(BF16)
            return carry

        lax.fori_loop(0, NY // 2, one, 0)

    pulls[2].wait()
    order_rows(early_ref, xe)

    def turn(yb, carry):
        xt[yb, 0] = xe[yb].astype(F32).T.astype(BF16)
        return carry

    lax.fori_loop(0, NY, turn, 0)

    def x_send(k):
        send(("xz", k), xt.at[t, 0], xt.at[t, k], zdev(-k))

    pair = {"tp": t + 1 - 2 * lax.rem(t, 2)}

    def x_take(j):
        blk = xt.at[t, j]
        got(("xz", j), blk)
        for k in (2, 6):
            send(("xx", k, j), blk, blk, tdev(k))
        send(("xc", 0, j), blk, blk, pair)

    def x_mid(j):
        got(("xx", 2, j), xt.at[0, pl.ds(0, 2)])
        for k, h in ((2, 0), (6, 128)):
            row = lax.rem(t + NT - k, NT)
            blk = xt.at[row, j]
            half = xt.at[row, j, pl.ds(h, 128)]
            send(("xf", k, j), half, half, tdev(k))
            send(("xc", k, j), blk, blk, pair)

    def x_far(j):
        row = lax.rem(t + 4, NT)
        blk = xt.at[row, j]
        got(("xf", 2, j), blk)
        send(("xc", 4, j), blk, blk, pair)

    def x_last():
        got(("xc", 0, 1), xt.at[pl.ds(0, 4), pl.ds(0, 3)])

    def a1_near(p):
        got(("a1", p, 1), wide[p].at[0, pl.ds(0, 128)])

    def a1_far(p):
        got(("a1", p, 2), wide[p].at[0, pl.ds(0, 64)])

    def a2_last(d):
        return (0, 1) if d == 1 else (2, 3)

    def a2_take(p, s, qs):
        for q in qs:
            got(("a2", p, 1, s - 1, q), wide[p].at[0, pl.ds(0, 64 if s == 4 else 128)])
            for d in (1, -1):
                blk = wide[p].at[yat(-d * s), wrow(zrow(q), 0, 64)]
                if s < 3 or (s == 3 and q in a2_last(d)):
                    send(("a2", p, d, s, q), blk, blk, ydev(d))

    def b1_take(s):
        got(("b1", 1, s - 1, 0), wb.at[0, pl.ds(0, 64 if s == 4 else 128)])
        for d in (1, -1):
            mine = 0 if d == 1 else 1
            for h in (mine, 1 - mine):
                blk = wb.at[yat(-d * s), wrow(z, 32 * h, 32)]
                if s < 3 or (s == 3 and h == mine):
                    send(("b1", d, s, h), blk, blk, ydev(d))
        for e in ordinals(s):
            blk = wb.at[yat(-e), own]
            for k in (1, -1):
                send(("b2", e, k), blk, blk, ring(k))

    def ordinals(s):
        return (0,) if s == 0 else ((4,) if s == 4 else (s, -s))

    def b2_take(s):
        got(("b2", s, 1), wb.at[0, pl.ds(0, 128 * len(ordinals(s)))])
        for e in ordinals(s):
            for k in (1, -1):
                yb = yat(-e)
                half = wb.at[yb, wrow(zat(-k), 0 if k == 1 else 32, 32)]
                send(("b2f", e, k), half, half, ring(k))

    def b2f_take(s):
        got(("b2f", s, 1), wb.at[0, pl.ds(0, 64 * len(ordinals(s)))])

    def project(w, first, width, yb, start):
        rows = xe[yb]

        def tile(c0, n):
            cols = pl.ds(first + c0, n)
            part = jnp.dot(rows, w[yb, :, pl.ds(c0, n)], preferred_element_type=F32)
            pre[:, cols] = part if start else pre[:, cols] + part

        def one(c, carry):
            tile(al(c * 256, 256), 256)
            return carry

        lax.fori_loop(0, width // 256, one, 0)
        if width % 256:
            tile(width - width % 256, width % 256)

    def late_project(w, first, c0, n):
        v = jnp.dot(xl[0], w[0, :, c0 : c0 + n], preferred_element_type=F32)
        for yb in range(1, NY):
            v = v + jnp.dot(xl[yb], w[yb, :, c0 : c0 + n], preferred_element_type=F32)
        prel[:, first + c0 : first + c0 + n] = v

    def project_a(s):
        for e in ordinals(s):
            project(wa, 0, CA, yat(-e), s == 0)

    def project_c(s):
        for e in ordinals(s):
            project(wc, CA, CC, yat(-e), s == 0)

    def project_b(s):
        for e in ordinals(s):
            project(wb, AC, CB, yat(-e), s == 0)

    def join_taps():
        for n in range(7, 11):
            pulls[n].wait()
        for n in range(5):
            cols = slice(n * LANE, (n + 1) * LANE)
            for src, pos in ((gt_ref, GPOS[n]), (ut_ref, UPOS[n])):
                taps_ref[0:3, pos * LANE : (pos + 1) * LANE] = src[:, cols].astype(F32)
        taps_ref[0:3, 768:832] = gt_ref[:, 640:HALF].astype(F32)
        taps_ref[0:3, 832:AC] = ut_ref[:, 640:HALF].astype(F32)

    def turn_cot():
        for n in range(5):
            v = cot_ref[n * LANE : (n + 1) * LANE, :].astype(F32).T
            cot[:, n * LANE : (n + 1) * LANE] = v.astype(BF16)
        cot[:, 640:768] = jnp.zeros((ROWS, LANE), BF16)
        cot[:, 640:HALF] = cot_ref[640:HALF, :].astype(F32).T.astype(BF16)

    def tap(cols):
        return [taps_ref[j : j + 1, cols] for j in range(3)]

    def mixed(src, cols):
        v = src[:, cols].astype(BF16).astype(F32)
        w = tap(cols)
        return v, w[0] * later(v, 2) + w[1] * later(v, 1) + w[2] * v, w

    def back(d, v, w, cols, i, q):
        r = (w[2] * d + w[1] * sooner(d, 1) + w[0] * sooner(d, 2)).astype(BF16)
        dpre[:, cols] = r
        dpq[i, q] = r
        for j, u in enumerate((later(v, 2), later(v, 1), v)):
            tsum[q, i, j : j + 1, :] = jnp.sum(d * u, axis=0, keepdims=True) * scale

    def tile_cols(n):
        return pl.ds(al(n * LANE, LANE), LANE)

    tsum[...] = jnp.zeros_like(tsum)
    dpq[2, 3] = jnp.zeros((ROWS, LANE), BF16)

    def early_pair(n, gpos, upos, i, q):
        gc, uc = tile_cols(gpos), tile_cols(upos)
        gv, gm, gw_ = mixed(pre, gc)
        uv, um, uw_ = mixed(pre, uc)
        c = cot[:, tile_cols(n)].astype(F32)
        act, th = gelu_parts(gm)
        back(c * um * gelu_slope(gm, th), gv, gw_, gc, i, q)
        back(c * act, uv, uw_, uc, i, q + 1)

    def early_a(n, carry):
        early_pair(n, 2 * n, 2 * n + 1, 0, 2 * n)
        return carry

    def early_b(m, carry):
        early_pair(m + 3, 2 * m + 7, 2 * m + 8, 1, 2 * m)
        return carry

    last = slice(768, AC)

    def early_c():
        early_pair(2, 4, 5, 2, 0)
        mv, mm, mw = mixed(pre, last)
        c = cot[:, 640:768].astype(F32)
        act, th = gelu_parts(mm)
        dg = c * swap_halves(mm) * gelu_slope(mm, th)
        du = swap_halves(c * act)
        back(jnp.where(low_lanes(dg.shape), dg, du), mv, mw, last, 2, 2)
        for k in range(1, NZ):
            send(("tz", k), tsum.at[zat(-k)], tzr.at[k], zdev(-k))

    def dp_send(i):
        for k in range(1, NZ):
            send(("dp", i, k), dpq.at[i, zat(-k)], dpg.at[i, k], zdev(-k))
        dpg[i, 0] = dpq[i, z]

    def dx(yb, carry):
        nt = (((1,), (1,)), ((), ()))
        v = lax.dot_general(dpre[:, 0:CA], wa[yb], nt, preferred_element_type=F32)
        v = v + lax.dot_general(dpre[:, CA:AC], wc[yb], nt, preferred_element_type=F32)
        v = v + lax.dot_general(dpre[:, AC:WIDE], wb[yb], nt, preferred_element_type=F32)
        dxp[:, pl.ds(al(yb * 256, 256), 256)] = v.astype(BF16)
        return carry

    def strip(tt):
        return pl.ds(al(tt * 32, 32), 32)

    core = lax.rem(t, 2)

    def dx_send():
        for x in range(4):
            send(("dc", x), dxp.at[strip(2 * x + 1 - core)], dxc.at[x], pair)

    def dx_pair():
        got(("dc", 0), dxc)
        for x in range(4):
            v = dxp[strip(2 * x + core), :].astype(F32) + dxc[x].astype(F32)
            dxs[x] = v.astype(BF16)
        for k in (2, 6, 4):
            to = lax.div(lax.rem(t + NT - k, NT), 2)
            send(("dx", k), dxs.at[to], dxr.at[k // 2], tdev(-k))

    def taps_first():
        got(("tz", 1), tzr.at[pl.ds(1, 3)])
        tys[...] = tsum[z] + tzr[1] + tzr[2] + tzr[3]
        for k in range(1, NY):
            send(("ty", k), tys, tyr.at[k], ydev(-k))

    def term(i, yb):
        v = jnp.dot(xt[yb, 0], dpg[i, 0], preferred_element_type=F32)
        for k in range(1, NZ):
            v = v + jnp.dot(xt[yb, k], dpg[i, k], preferred_element_type=F32)
        return v * scale

    def side(d):
        return 0 if d == 1 else 1

    def part(d):
        return pl.ds(0, 128) if d == 1 else pl.ds(128, 128)

    def rs(i, s):
        if s == 0:
            got(("dp", i, 1), dpg.at[i, pl.ds(1, 3)])
            for d in (1, -1):
                buf = snd.at[side(d), i, 0]
                buf[...] = term(i, yat(3 * d)).astype(BF16)
                send(("rs", i, 0, d), buf, rcv.at[side(d), i, 0], ydev(d))
            v = term(i, yat(4))
            for d in (1, -1):
                buf = snd.at[side(d), i, 3, part(d)]
                buf[...] = (v[0:128] if d == 1 else v[128:256]).astype(BF16)
                send(("rs", i, 3, d), buf, rcv.at[side(d), i, 3, part(d)], ydev(2 * d))
            return
        if s < 3:
            for d in (1, -1):
                v = term(i, yat(d * (3 - s)))
                if s == 1:
                    got(("rs", i, 0, d), xt.at[0, 0, pl.ds(0, 192)])
                else:
                    got(("rs", i, s - 1, d), rcv.at[side(d), i, s - 1])
                v = v + rcv[side(d), i, s - 1].astype(F32)
                buf = snd.at[side(d), i, s]
                if s == 1:
                    w = rcv[side(d), i, 3, part(d), :].astype(F32)
                    if d == 1:
                        buf[0:128, :] = (v[0:128] + w).astype(BF16)
                        buf[128:256, :] = v[128:256].astype(BF16)
                    else:
                        buf[0:128, :] = v[0:128].astype(BF16)
                        buf[128:256, :] = (v[128:256] + w).astype(BF16)
                else:
                    buf[...] = v.astype(BF16)
                send(("rs", i, s, d), buf, rcv.at[side(d), i, s], ydev(d))
            return
        v = term(i, y)
        for d in (1, -1):
            got(("rs", i, 2, d), rcv.at[side(d), i, 2])
            v = v + rcv[side(d), i, 2].astype(F32)
        fin[i] = v.astype(BF16)
        for k in range(1, NZ):
            send(("fin", i, k), fin.at[i, wrow(zat(-k), 0, 64)], finr.at[k, i], zdev(-k))
        finr[0, i] = fin[i, own, :]

    def eg_own():
        return pltpu.make_async_copy(egs, eg_ref.at[strip(t)], lsem.at[11])

    def hid_flush():
        return pltpu.make_async_copy(hid_ref, hid_out, lsem.at[12])

    def dx_reduce():
        v = dxs[lax.div(t, 2)].astype(F32)
        got(("dx", 2), dxr.at[pl.ds(1, 3)])
        for k in (2, 6, 4):
            v = v + dxr[k // 2].astype(F32)
        for yp in range(NY // 2):
            for zp in range(2):
                a = v[:, 2 * yp * 256 + zp * LANE : 2 * yp * 256 + (zp + 1) * LANE]
                b = v[:, (2 * yp + 1) * 256 + zp * LANE : (2 * yp + 1) * 256 + (zp + 1) * LANE]
                low = low_lanes(a.shape)
                at0 = 2 * zp * 512 + yp * LANE
                egs[:, at0 : at0 + LANE] = jnp.where(low, a, swap_halves(b)).astype(BF16)
                egs[:, at0 + 512 : at0 + 512 + LANE] = jnp.where(low, swap_halves(a), b).astype(BF16)
        for k in (2, 6, 4):
            send(("eg", k), egs, eg_ref.at[strip(t)], tdev(k))
        send(("ec", 0), egs, eg_ref.at[strip(t)], pair)
        eg_own().start()

    def eg_cross():
        got(("eg", 2), dxr.at[pl.ds(1, 3)])
        for k in (2, 6, 4):
            here = eg_ref.at[strip(lax.rem(t + NT - k, NT))]
            send(("ec", k), here, here, pair)

    def eg_last():
        got(("ec", 0), dxc)

    def taps_finish():
        v = tys[...]
        got(("ty", 1), tyr.at[pl.ds(1, 7)])
        for k in range(1, NY):
            v = v + tyr[k]
        tfr[0] = v
        for k in range(1, NZ):
            send(("tf", k), tfr.at[0], tfr.at[k], zdev(-k))

    def late_pair(n, gpos, upos):
        _, gm, _ = mixed(prel, tile_cols(gpos))
        _, um, _ = mixed(prel, tile_cols(upos))
        act, _ = gelu_parts(gm)
        hid_ref[tile_cols(n), :] = (act * um).T.astype(BF16)

    def late_a(n, carry):
        late_pair(n, 2 * n, 2 * n + 1)
        return carry

    def late_b(m, carry):
        late_pair(m + 3, 2 * m + 7, 2 * m + 8)
        return carry

    def late_c():
        late_pair(2, 4, 5)
        _, mm, _ = mixed(prel, last)
        act, _ = gelu_parts(mm)
        hid_ref[640:HALF, :] = (act * swap_halves(mm)).T[0:64].astype(BF16)

    b1_take(1)
    a1_near("a")
    a2_own("a", 1)
    a2_own("a", 2)
    a2_take("a", 1, (0,))
    a1_far("a")
    a2_own("a", 3)
    b2_take(0)
    x_send(1)
    a2_take("a", 1, (1,))
    b1_take(2)
    x_send(2)
    a2_take("a", 1, (2,))
    a2_take("a", 1, (3,))
    b2_take(1)
    x_send(3)
    pulls[3].wait()
    order_rows(late_ref, xl)
    b1_take(3)
    a2_take("a", 2, (0, 1))
    project_a(0)
    a2_take("a", 2, (2, 3))
    b2_take(2)
    b1_take(4)
    x_take(1)
    a1_near("c")
    a1_far("c")
    a2_take("a", 3, (0,))
    a2_own("c", 0)
    project_a(1)
    a2_take("a", 3, (1,))
    a2_own("c", 1)
    a2_take("a", 3, (2,))
    a2_own("c", 2)
    a2_take("a", 3, (3,))
    a2_own("c", 3)
    x_take(2)
    project_a(2)
    a2_take("c", 1, (0,))
    a2_take("c", 1, (1,))
    x_take(3)
    a2_take("c", 1, (2,))
    project_a(3)
    b2_take(3)
    a2_take("c", 1, (3,))
    a2_take("a", 4, range(NZ))
    x_mid(1)
    b2_take(4)
    a2_take("c", 2, (0,))
    project_a(4)
    x_mid(2)
    a2_take("c", 2, (1,))
    pulls[4].wait()
    turn_cot()
    join_taps()
    lax.fori_loop(0, 2, early_a, 0)
    dp_send(0)
    a2_take("c", 2, (2,))
    b2f_take(0)
    project_b(0)
    x_far(1)
    a2_take("c", 2, (3,))
    b2f_take(1)
    project_b(1)
    x_mid(3)
    b2f_take(2)
    project_b(2)
    a2_take("c", 3, (0,))
    x_far(2)
    b2f_take(3)
    project_b(3)
    a2_take("c", 3, (1,))
    b2f_take(4)
    project_b(4)
    a2_take("c", 3, (2, 3))
    lax.fori_loop(0, 2, early_b, 0)
    dp_send(1)
    x_far(3)
    project_c(0)
    project_c(1)
    project_c(2)
    project_c(3)
    x_last()
    rs(0, 0)
    a2_take("c", 4, range(NZ))
    project_c(4)
    early_c()
    dp_send(2)
    lax.fori_loop(0, NY, dx, 0)
    dx_send()
    rs(1, 0)
    rs(0, 1)
    dx_pair()
    taps_first()
    rs(2, 0)
    rs(0, 2)
    rs(1, 1)
    late_project(wa, 0, 0, 256)
    late_project(wa, 0, 256, 256)
    late_project(wc, CA, 0, 256)
    late_project(wc, CA, 256, 128)
    rs(2, 1)
    dx_reduce()
    rs(0, 3)
    rs(1, 2)
    late_project(wb, AC, 0, 256)
    rs(2, 2)
    rs(1, 3)
    taps_finish()
    late_project(wb, AC, 256, 256)
    eg_cross()
    rs(2, 3)
    lax.fori_loop(0, 2, late_a, 0)
    lax.fori_loop(0, 2, late_b, 0)
    late_c()
    hid_flush().start()

    def spread(pos, v, prev, nxt):
        (gs, us), (gn, un) = prev, nxt
        if pos == 6:
            gn[:, 640:HALF] = gs[:, 640:HALF] + v[:, 0:64]
            un[:, 640:HALF] = us[:, 640:HALF] + swap_halves(v)[:, 0:64]
            return
        side_, n = (0, GPOS.index(pos)) if pos in GPOS else (1, UPOS.index(pos))
        cols = slice(n * LANE, (n + 1) * LANE)
        nxt[side_][:, cols] = prev[side_][:, cols] + v

    def tile_out(pos, v):
        spread(pos, v, (gsum_ref, usum_ref), (gnext_ref, unext_ref))

    def taps_out(pos, v):
        if pos == 6:
            gtnext_ref[:, 640:HALF] = gtsum_ref[:, 640:HALF] + v[0:3, 0:64]
            utnext_ref[:, 640:HALF] = utsum_ref[:, 640:HALF] + swap_halves(v)[0:3, 0:64]
            return
        spread(pos, v[0:3], (gtsum_ref, utsum_ref), (gtnext_ref, utnext_ref))

    def tf_take():
        got(("tf", 1), tfr.at[pl.ds(1, 3)])

    def fin_take(i):
        got(("fin", i, 1), finr.at[pl.ds(1, 3), i])

    def write_out(i):
        tiles = ((0, 1, 2, 3), (7, 8, 9, 10), (4, 5, 6))[i]
        for q, n in enumerate(tiles):
            k = lax.rem(q + NZ - z, NZ)
            tile_out(n, finr[k, i].astype(F32))
            taps_out(n, tfr[k, i])

    def sends_done():
        eg_own().wait()
        hid_flush().wait()
        gone("a1a", wa.at[0, pl.ds(0, 192)])
        gone("a1c", wc.at[0, pl.ds(0, 192)])
        gone("a2a", wa.at[pl.ds(0, 7)])
        gone("a2c", wc.at[pl.ds(0, 7)])
        gone("b1", wb.at[pl.ds(0, 7), pl.ds(0, 64)])
        gone("b2", wb.at[pl.ds(0, 4)])
        gone("b2f", wb.at[pl.ds(0, 2)])
        gone("x", xt.at[pl.ds(0, 6)])
        gone("rs", xt.at[pl.ds(0, 5), pl.ds(0, 3)])
        gone("fin", finr.at[pl.ds(0, 3)])
        gone("t", tyr.at[pl.ds(0, 6)])
        gone("ty", tyr.at[pl.ds(0, 7)])
        gone("d", xt.at[pl.ds(0, 7), pl.ds(0, 2)])

    pulls[5].wait()
    pulls[6].wait()
    tf_take()
    fin_take(0)
    write_out(0)
    fin_take(1)
    write_out(1)
    eg_last()
    fin_take(2)
    write_out(2)
    sends_done()


def flush(*refs):
    sem = refs[12]
    copies = [pltpu.make_async_copy(refs[n], refs[6 + n], sem.at[n]) for n in (1, 0, 2, 3, 4, 5)]
    for c in copies:
        c.start()
    for c in copies:
        c.wait()


def per_device(
    late_rows,
    early_rows,
    hidden_cot,
    gate_weight,
    up_weight,
    gate_taps,
    up_taps,
    gate_grad_sum,
    up_grad_sum,
    gate_taps_sum,
    up_taps_sum,
):
    vmem = pl.BlockSpec(memory_space=pltpu.VMEM)
    shapes = (
        ((HALF, ROWS), BF16),
        ((ROWS, 2048), BF16),
        ((64, HALF), F32),
        ((64, HALF), F32),
        ((3, HALF), F32),
        ((3, HALF), F32),
    )
    n_sem = 91
    hbm = pl.BlockSpec(memory_space=pltpu.HBM)
    hid, *rest = pl.pallas_call(
        kernel,
        out_shape=[pltpu.VMEM(s, d) for s, d in shapes],
        in_specs=[hbm] * 11,
        out_specs=[pl.BlockSpec(memory_space=pl.ANY)] * 2 + [vmem] * 4,
        scratch_shapes=[
            pltpu.VMEM((HALF, ROWS), BF16),
            pltpu.VMEM((ROWS, 2048), BF16),
            pltpu.VMEM((ROWS, 2048), BF16),
            pltpu.VMEM((HALF, ROWS), BF16),
            pltpu.VMEM((64, HALF), BF16),
            pltpu.VMEM((64, HALF), BF16),
            pltpu.VMEM((64, HALF), F32),
            pltpu.VMEM((64, HALF), F32),
            pltpu.VMEM((3, HALF), BF16),
            pltpu.VMEM((3, HALF), BF16),
            pltpu.VMEM((3, HALF), F32),
            pltpu.VMEM((3, HALF), F32),
            pltpu.VMEM((64, LANE), F32),
            pltpu.VMEM((8, WIDE), F32),
            pltpu.VMEM((NY, 256, CA), BF16),
            pltpu.VMEM((NY, 256, CC), BF16),
            pltpu.VMEM((NY, 256, CB), BF16),
            pltpu.VMEM((NY, ROWS, 256), BF16),
            pltpu.VMEM((NY, ROWS, 256), BF16),
            pltpu.VMEM((NY, NZ, 256, ROWS), BF16),
            pltpu.VMEM((ROWS, WIDE), F32),
            pltpu.VMEM((ROWS, WIDE), F32),
            pltpu.VMEM((ROWS, 768), BF16),
            pltpu.VMEM((ROWS, WIDE), BF16),
            pltpu.VMEM((3, NZ, ROWS, LANE), BF16),
            pltpu.VMEM((3, NZ, ROWS, LANE), BF16),
            pltpu.VMEM((2, 3, 4, 256, LANE), BF16),
            pltpu.VMEM((2, 3, 4, 256, LANE), BF16),
            pltpu.VMEM((3, 256, LANE), BF16),
            pltpu.VMEM((NZ, 3, 64, LANE), BF16),
            pltpu.VMEM((ROWS, 2048), BF16),
            pltpu.VMEM((4, 32, 2048), BF16),
            pltpu.VMEM((4, 32, 2048), BF16),
            pltpu.VMEM((4, 32, 2048), BF16),
            pltpu.VMEM((32, 2048), BF16),
            pltpu.VMEM((NZ, 3, 8, LANE), F32),
            pltpu.VMEM((NZ, 3, 8, LANE), F32),
            pltpu.VMEM((3, 8, LANE), F32),
            pltpu.VMEM((NY, 3, 8, LANE), F32),
            pltpu.VMEM((NZ, 3, 8, LANE), F32),
            pltpu.SemaphoreType.DMA((13,)),
            pltpu.SemaphoreType.DMA((13,)),
            pltpu.SemaphoreType.DMA((n_sem,)),
        ],
        compiler_params=pltpu.CompilerParams(
            collective_id=0, has_side_effects=True, vmem_limit_bytes=57000 * 1024
        ),
    )(
        late_rows,
        early_rows,
        hidden_cot.T,
        gate_weight,
        up_weight,
        gate_grad_sum,
        up_grad_sum,
        gate_taps,
        up_taps,
        gate_taps_sum,
        up_taps_sum,
    )
    hid, *rest = pl.pallas_call(
        flush,
        out_shape=[jax.ShapeDtypeStruct(s, d) for s, d in shapes],
        in_specs=[vmem] * 6,
        out_specs=[hbm] * 6,
        scratch_shapes=[pltpu.SemaphoreType.DMA((6,))],
        compiler_params=pltpu.CompilerParams(vmem_limit_bytes=8 * 1024 * 1024),
    )(hid, *rest)
    return (hid.T, *rest)


def solution(mesh):
    split = Mesh(
        mesh.devices.reshape(mesh.shape["rep"], NZ, NY, mesh.shape["tp"]),
        ("rep", "fs_0", "fs_1", "tp"),
    )
    placed = (
        P(REP_FS, None),
        P(REP_FS, None),
        P(REP_FS, "tp"),
        P(FS, "tp"),
        P(FS, "tp"),
        P(None, "tp"),
        P(None, "tp"),
        P(REP_FS, "tp"),
        P(REP_FS, "tp"),
        P("rep", "tp"),
        P("rep", "tp"),
    )
    return jax.shard_map(
        per_device,
        mesh=split,
        in_specs=placed,
        out_specs=(
            P(REP_FS, "tp"),
            P(REP_FS, None),
            P(REP_FS, "tp"),
            P(REP_FS, "tp"),
            P("rep", "tp"),
            P("rep", "tp"),
        ),
        check_vma=False,
    )
```

```python
import jax
import jax.numpy as jnp
from jax import lax
from jax.experimental import pallas as pl
from jax.experimental.pallas import tpu as pltpu
from jax.sharding import Mesh
from jax.sharding import PartitionSpec as P

FS = ("fs_0", "fs_1")
REP_FS = ("rep", "fs_0", "fs_1")
MESH = pl.DeviceIdType.MESH

NZ, NY, NT = 4, 8, 8
ROWS = 256
LANE = 128
CA, CC, CB = 512, 384, 512
AC = CA + CC
WIDE = AC + CB
HALF = 704
GPOS, UPOS = (0, 2, 4, 7, 9), (1, 3, 5, 8, 10)
F32, BF16 = jnp.float32, jnp.bfloat16
GELU_K = 0.7978845608028654
GELU_A = 0.044715


def al(v, m):
    return pl.multiple_of(v, m)


def low_lanes(shape):
    return lax.broadcasted_iota(jnp.int32, shape, 1) < 64


def swap_halves(v):
    return pltpu.roll(v, 64, 1)


def row_of(shape):
    return lax.broadcasted_iota(jnp.int32, shape, 0)


def later(v, by):
    return jnp.where(row_of(v.shape) >= by, pltpu.roll(v, by, 0), 0.0)


def sooner(v, by):
    n = v.shape[0]
    return jnp.where(row_of(v.shape) < n - by, pltpu.roll(v, n - by, 0), 0.0)


def gelu_parts(v):
    t = jnp.tanh(GELU_K * (v + GELU_A * v * v * v))
    return 0.5 * v * (1.0 + t), t


def gelu_slope(v, t):
    return 0.5 * (1.0 + t) + 0.5 * v * (1.0 - t * t) * GELU_K * (1.0 + 3.0 * GELU_A * v * v)


def kernel(
    late_hbm,
    early_hbm,
    cot_hbm,
    gw_hbm,
    uw_hbm,
    gsum_hbm,
    usum_hbm,
    gt_hbm,
    ut_hbm,
    gtsum_hbm,
    utsum_hbm,
    hid_out,
    eg_ref,
    gnext_ref,
    unext_ref,
    gtnext_ref,
    utnext_ref,
    hid_ref,
    late_ref,
    early_ref,
    cot_ref,
    gw,
    uw,
    gsum_ref,
    usum_ref,
    gt_ref,
    ut_ref,
    gtsum_ref,
    utsum_ref,
    wmix,
    taps_ref,
    wa,
    wc,
    wb,
    xe,
    xl,
    xt,
    pre,
    prel,
    cot,
    dpre,
    dpq,
    dpg,
    snd,
    rcv,
    fin,
    finr,
    dxp,
    dxc,
    dxs,
    dxr,
    egs,
    tsum,
    tzr,
    tys,
    tyr,
    tfr,
    lsem,
    ssem,
    rsem,
):
    rep = lax.axis_index("rep")
    z = lax.axis_index("fs_0")
    y = lax.axis_index("fs_1")
    t = lax.axis_index("tp")
    scale = (NZ * NY * ROWS) ** -0.5

    def ring(k):
        g = lax.rem(rep * NZ + z + 2 * NZ + k, 2 * NZ)
        return {"rep": lax.div(g, NZ), "fs_0": lax.rem(g, NZ)}

    def zdev(k):
        return {"fs_0": lax.rem(z + NZ + k, NZ)}

    def ydev(k):
        return {"fs_1": lax.rem(y + NY + k, NY)}

    def tdev(k):
        return {"tp": lax.rem(t + NT + k, NT)}

    def zat(k):
        return lax.rem(z + NZ + k, NZ)

    def yat(k):
        return lax.rem(y + NY + k, NY)

    peers = [ring(1), ring(-1), ring(2), ring(-2)]
    peers += [zdev(k) for k in range(1, NZ)]
    peers += [ydev(k) for k in range(1, NY)]
    peers += [tdev(k) for k in range(1, NT)]

    barrier = pltpu.get_barrier_semaphore()
    for dev in peers:
        pl.semaphore_signal(barrier, inc=1, device_id=dev, device_id_type=MESH)

    pulls = []
    for n, (src, dst) in enumerate(
        (
            (gw_hbm, gw),
            (uw_hbm, uw),
            (early_hbm, early_ref),
            (late_hbm, late_ref),
            (cot_hbm, cot_ref),
            (gsum_hbm, gsum_ref),
            (usum_hbm, usum_ref),
            (gt_hbm, gt_ref),
            (ut_hbm, ut_ref),
            (gtsum_hbm, gtsum_ref),
            (utsum_hbm, utsum_ref),
        )
    ):
        c = pltpu.make_async_copy(src, dst, lsem.at[n])
        c.start()
        pulls.append(c)

    arrivals, kinds = {}, {}

    def arrival(name):
        kind, rest = name[0], name[1:]
        if kind == "a1":
            rest = (rest[0], abs(rest[1]))
        elif kind == "a2":
            rest = (rest[0], rest[2], rest[3])
        elif kind == "b1":
            rest = (rest[1],)
        elif kind in ("b2", "b2f"):
            rest = (abs(rest[0]),)
        elif kind in ("xx", "xf"):
            rest = (rest[1],)
        elif kind in ("dp", "fin"):
            rest = (rest[0],)
        elif kind == "rs":
            rest = (rest[0], rest[1] % 3, rest[2])
        elif kind != "xz":
            rest = ()
        return arrivals.setdefault((kind, *rest), len(arrivals))

    def kind_of(name):
        kind = name[0]
        if kind in ("a1", "a2"):
            kind += name[1]
        elif kind in ("xz", "xx", "xf", "xc"):
            kind = "x"
        elif kind in ("dc", "dx", "eg", "ec"):
            kind = "d"
        elif kind in ("tz", "tf"):
            kind = "t"
        elif kind == "dp":
            kind = "rs"
        return kinds.setdefault(kind, len(kinds))

    def copy_of(src, dst, s, r, dev):
        return pltpu.make_async_remote_copy(
            src_ref=src,
            dst_ref=dst,
            send_sem=ssem.at[s],
            recv_sem=rsem.at[r],
            device_id=dev,
            device_id_type=MESH,
        )

    def send(name, src, dst, dev):
        copy_of(src, dst, kind_of(name), arrival(name), dev).start()

    def got(name, ref):
        copy_of(ref, ref, 0, arrival(name), ydev(1)).wait_recv()

    def gone(kind, ref):
        copy_of(ref, ref, kinds[kind], 0, ydev(1)).wait_send()

    def wrow(zz, first, n):
        return pl.ds(al(zz * 64 + first, 32), n)

    own = wrow(z, 0, 64)

    pulls[0].wait()
    pulls[1].wait()
    wmix[:, 0:64] = gw[:, 640:HALF].astype(F32)
    wmix[:, 64:LANE] = uw[:, 640:HALF].astype(F32)
    wc[y, own, 256:CC] = wmix[...].astype(BF16)
    for n in range(5):
        cols = slice(n * LANE, (n + 1) * LANE)
        for src, pos in ((gw, GPOS[n]), (uw, UPOS[n])):
            here = slice(pos * LANE, (pos + 1) * LANE)
            if pos < 4:
                wa[y, own, here] = src[:, cols]
            elif pos < 7:
                wc[y, own, (pos - 4) * LANE : (pos - 3) * LANE] = src[:, cols]
            else:
                wb[y, own, (pos - 7) * LANE : (pos - 6) * LANE] = src[:, cols]
    pl.semaphore_wait(barrier, len(peers))

    def zrow(q):
        return zat((0, -1, 1, 2)[q])

    wide = {"a": wa, "c": wc}

    def a2_own(p, q):
        blk = wide[p].at[y, wrow(zrow(q), 0, 64)]
        for d in (1, -1):
            send(("a2", p, d, 0, q), blk, blk, ydev(d))

    def a1_send(p, near):
        if near:
            blk = wide[p].at[y, own]
            for k in (1, -1):
                send(("a1", p, k), blk, blk, ring(k))
            return
        for h, k in ((0, 2), (1, -2)):
            blk = wide[p].at[y, wrow(z, 32 * h, 32)]
            send(("a1", p, k), blk, blk, ring(k))

    b_own = wb.at[y, own]
    a1_send("a", True)
    for h, d in ((0, 1), (1, -1), (1, 1), (0, -1)):
        blk = wb.at[y, wrow(z, 32 * h, 32)]
        send(("b1", d, 0, h), blk, blk, ydev(d))
    a1_send("a", False)
    a2_own("a", 0)
    for k in (1, -1):
        send(("b2", 0, k), b_own, b_own, ring(k))
    a1_send("c", True)
    a1_send("c", False)

    def order_rows(src_ref, dst):
        def one(yp, carry):
            for zp in range(2):
                a = src_ref[:, pl.ds(al(2 * zp * 512 + yp * LANE, LANE), LANE)].astype(F32)
                b = src_ref[:, pl.ds(al((2 * zp + 1) * 512 + yp * LANE, LANE), LANE)].astype(F32)
                low = low_lanes(a.shape)
                cols = slice(zp * LANE, (zp + 1) * LANE)
                dst[2 * yp, :, cols] = jnp.where(low, a, swap_halves(b)).astype(BF16)
                dst[2 * yp + 1, :, cols] = jnp.where(low, swap_halves(a), b).astype(BF16)
            return carry

        lax.fori_loop(0, NY // 2, one, 0)

    pulls[2].wait()
    order_rows(early_ref, xe)

    def turn(yb, carry):
        xt[yb, 0] = xe[yb].astype(F32).T.astype(BF16)
        return carry

    lax.fori_loop(0, NY, turn, 0)

    def x_send(k):
        send(("xz", k), xt.at[t, 0], xt.at[t, k], zdev(-k))

    pair = {"tp": t + 1 - 2 * lax.rem(t, 2)}

    def x_take(j):
        blk = xt.at[t, j]
        got(("xz", j), blk)
        for k in (2, 6):
            send(("xx", k, j), blk, blk, tdev(k))
        send(("xc", 0, j), blk, blk, pair)

    def x_mid(j):
        got(("xx", 2, j), xt.at[0, pl.ds(0, 2)])
        for k, h in ((2, 0), (6, 128)):
            row = lax.rem(t + NT - k, NT)
            blk = xt.at[row, j]
            half = xt.at[row, j, pl.ds(h, 128)]
            send(("xf", k, j), half, half, tdev(k))
            send(("xc", k, j), blk, blk, pair)

    def x_far(j):
        row = lax.rem(t + 4, NT)
        blk = xt.at[row, j]
        got(("xf", 2, j), blk)
        send(("xc", 4, j), blk, blk, pair)

    def x_last():
        got(("xc", 0, 1), xt.at[pl.ds(0, 4), pl.ds(0, 3)])

    def a1_near(p):
        got(("a1", p, 1), wide[p].at[0, pl.ds(0, 128)])

    def a1_far(p):
        got(("a1", p, 2), wide[p].at[0, pl.ds(0, 64)])

    def a2_last(d):
        return (0, 1) if d == 1 else (2, 3)

    def a2_take(p, s, qs):
        for q in qs:
            got(("a2", p, 1, s - 1, q), wide[p].at[0, pl.ds(0, 64 if s == 4 else 128)])
            for d in (1, -1):
                blk = wide[p].at[yat(-d * s), wrow(zrow(q), 0, 64)]
                if s < 3 or (s == 3 and q in a2_last(d)):
                    send(("a2", p, d, s, q), blk, blk, ydev(d))

    def b1_take(s):
        got(("b1", 1, s - 1, 0), wb.at[0, pl.ds(0, 64 if s == 4 else 128)])
        for d in (1, -1):
            mine = 0 if d == 1 else 1
            for h in (mine, 1 - mine):
                blk = wb.at[yat(-d * s), wrow(z, 32 * h, 32)]
                if s < 3 or (s == 3 and h == mine):
                    send(("b1", d, s, h), blk, blk, ydev(d))
        for e in ordinals(s):
            blk = wb.at[yat(-e), own]
            for k in (1, -1):
                send(("b2", e, k), blk, blk, ring(k))

    def ordinals(s):
        return (0,) if s == 0 else ((4,) if s == 4 else (s, -s))

    def b2_take(s):
        got(("b2", s, 1), wb.at[0, pl.ds(0, 128 * len(ordinals(s)))])
        for e in ordinals(s):
            for k in (1, -1):
                yb = yat(-e)
                half = wb.at[yb, wrow(zat(-k), 0 if k == 1 else 32, 32)]
                send(("b2f", e, k), half, half, ring(k))

    def b2f_take(s):
        got(("b2f", s, 1), wb.at[0, pl.ds(0, 64 * len(ordinals(s)))])

    def project(w, first, width, yb, start):
        rows = xe[yb]

        def tile(c0, n):
            cols = pl.ds(first + c0, n)
            part = jnp.dot(rows, w[yb, :, pl.ds(c0, n)], preferred_element_type=F32)
            pre[:, cols] = part if start else pre[:, cols] + part

        def one(c, carry):
            tile(al(c * 256, 256), 256)
            return carry

        lax.fori_loop(0, width // 256, one, 0)
        if width % 256:
            tile(width - width % 256, width % 256)

    def late_project(w, first, c0, n):
        v = jnp.dot(xl[0], w[0, :, c0 : c0 + n], preferred_element_type=F32)
        for yb in range(1, NY):
            v = v + jnp.dot(xl[yb], w[yb, :, c0 : c0 + n], preferred_element_type=F32)
        prel[:, first + c0 : first + c0 + n] = v

    def project_a(s):
        for e in ordinals(s):
            project(wa, 0, CA, yat(-e), s == 0)

    def project_c(s):
        for e in ordinals(s):
            project(wc, CA, CC, yat(-e), s == 0)

    def project_b(s):
        for e in ordinals(s):
            project(wb, AC, CB, yat(-e), s == 0)

    def join_taps():
        for n in range(7, 11):
            pulls[n].wait()
        for n in range(5):
            cols = slice(n * LANE, (n + 1) * LANE)
            for src, pos in ((gt_ref, GPOS[n]), (ut_ref, UPOS[n])):
                taps_ref[0:3, pos * LANE : (pos + 1) * LANE] = src[:, cols].astype(F32)
        taps_ref[0:3, 768:832] = gt_ref[:, 640:HALF].astype(F32)
        taps_ref[0:3, 832:AC] = ut_ref[:, 640:HALF].astype(F32)

    def turn_cot():
        for n in range(5):
            v = cot_ref[n * LANE : (n + 1) * LANE, :].astype(F32).T
            cot[:, n * LANE : (n + 1) * LANE] = v.astype(BF16)
        cot[:, 640:768] = jnp.zeros((ROWS, LANE), BF16)
        cot[:, 640:HALF] = cot_ref[640:HALF, :].astype(F32).T.astype(BF16)

    def tap(cols):
        return [taps_ref[j : j + 1, cols] for j in range(3)]

    def mixed(src, cols):
        v = src[:, cols].astype(BF16).astype(F32)
        w = tap(cols)
        return v, w[0] * later(v, 2) + w[1] * later(v, 1) + w[2] * v, w

    def back(d, v, w, cols, i, q):
        r = (w[2] * d + w[1] * sooner(d, 1) + w[0] * sooner(d, 2)).astype(BF16)
        dpre[:, cols] = r
        dpq[i, q] = r
        for j, u in enumerate((later(v, 2), later(v, 1), v)):
            tsum[q, i, j : j + 1, :] = jnp.sum(d * u, axis=0, keepdims=True) * scale

    def tile_cols(n):
        return pl.ds(al(n * LANE, LANE), LANE)

    tsum[...] = jnp.zeros_like(tsum)
    dpq[2, 3] = jnp.zeros((ROWS, LANE), BF16)

    def early_pair(n, gpos, upos, i, q):
        gc, uc = tile_cols(gpos), tile_cols(upos)
        gv, gm, gw_ = mixed(pre, gc)
        uv, um, uw_ = mixed(pre, uc)
        c = cot[:, tile_cols(n)].astype(F32)
        act, th = gelu_parts(gm)
        back(c * um * gelu_slope(gm, th), gv, gw_, gc, i, q)
        back(c * act, uv, uw_, uc, i, q + 1)

    def early_a(n, carry):
        early_pair(n, 2 * n, 2 * n + 1, 0, 2 * n)
        return carry

    def early_b(m, carry):
        early_pair(m + 3, 2 * m + 7, 2 * m + 8, 1, 2 * m)
        return carry

    last = slice(768, AC)

    def early_c():
        early_pair(2, 4, 5, 2, 0)
        mv, mm, mw = mixed(pre, last)
        c = cot[:, 640:768].astype(F32)
        act, th = gelu_parts(mm)
        dg = c * swap_halves(mm) * gelu_slope(mm, th)
        du = swap_halves(c * act)
        back(jnp.where(low_lanes(dg.shape), dg, du), mv, mw, last, 2, 2)
        for k in range(1, NZ):
            send(("tz", k), tsum.at[zat(-k)], tzr.at[k], zdev(-k))

    def dp_send(i):
        for k in range(1, NZ):
            send(("dp", i, k), dpq.at[i, zat(-k)], dpg.at[i, k], zdev(-k))
        dpg[i, 0] = dpq[i, z]

    def dx(yb, carry):
        nt = (((1,), (1,)), ((), ()))
        v = lax.dot_general(dpre[:, 0:CA], wa[yb], nt, preferred_element_type=F32)
        v = v + lax.dot_general(dpre[:, CA:AC], wc[yb], nt, preferred_element_type=F32)
        v = v + lax.dot_general(dpre[:, AC:WIDE], wb[yb], nt, preferred_element_type=F32)
        dxp[:, pl.ds(al(yb * 256, 256), 256)] = v.astype(BF16)
        return carry

    def strip(tt):
        return pl.ds(al(tt * 32, 32), 32)

    core = lax.rem(t, 2)

    def dx_send():
        for x in range(4):
            send(("dc", x), dxp.at[strip(2 * x + 1 - core)], dxc.at[x], pair)

    def dx_pair():
        got(("dc", 0), dxc)
        for x in range(4):
            v = dxp[strip(2 * x + core), :].astype(F32) + dxc[x].astype(F32)
            dxs[x] = v.astype(BF16)
        for k in (2, 6, 4):
            to = lax.div(lax.rem(t + NT - k, NT), 2)
            send(("dx", k), dxs.at[to], dxr.at[k // 2], tdev(-k))

    def taps_first():
        got(("tz", 1), tzr.at[pl.ds(1, 3)])
        tys[...] = tsum[z] + tzr[1] + tzr[2] + tzr[3]
        for k in range(1, NY):
            send(("ty", k), tys, tyr.at[k], ydev(-k))

    def term(i, yb):
        v = jnp.dot(xt[yb, 0], dpg[i, 0], preferred_element_type=F32)
        for k in range(1, NZ):
            v = v + jnp.dot(xt[yb, k], dpg[i, k], preferred_element_type=F32)
        return v * scale

    def side(d):
        return 0 if d == 1 else 1

    def part(d):
        return pl.ds(0, 128) if d == 1 else pl.ds(128, 128)

    def rs(i, s):
        if s == 0:
            got(("dp", i, 1), dpg.at[i, pl.ds(1, 3)])
            v = term(i, yat(4))
            for d in (1, -1):
                buf = snd.at[side(d), i, 3, part(d)]
                buf[...] = (v[0:128] if d == 1 else v[128:256]).astype(BF16)
                send(("rs", i, 3, d), buf, rcv.at[side(d), i, 3, part(d)], ydev(2 * d))
            for d in (1, -1):
                buf = snd.at[side(d), i, 0]
                buf[...] = term(i, yat(3 * d)).astype(BF16)
                send(("rs", i, 0, d), buf, rcv.at[side(d), i, 0], ydev(d))
            return
        if s < 3:
            for d in (1, -1):
                v = term(i, yat(d * (3 - s)))
                if s == 1:
                    got(("rs", i, 0, d), xt.at[0, 0, pl.ds(0, 192)])
                else:
                    got(("rs", i, s - 1, d), rcv.at[side(d), i, s - 1])
                v = v + rcv[side(d), i, s - 1].astype(F32)
                buf = snd.at[side(d), i, s]
                if s == 1:
                    w = rcv[side(d), i, 3, part(d), :].astype(F32)
                    if d == 1:
                        buf[0:128, :] = (v[0:128] + w).astype(BF16)
                        buf[128:256, :] = v[128:256].astype(BF16)
                    else:
                        buf[0:128, :] = v[0:128].astype(BF16)
                        buf[128:256, :] = (v[128:256] + w).astype(BF16)
                else:
                    buf[...] = v.astype(BF16)
                send(("rs", i, s, d), buf, rcv.at[side(d), i, s], ydev(d))
            return
        v = term(i, y)
        for d in (1, -1):
            got(("rs", i, 2, d), rcv.at[side(d), i, 2])
            v = v + rcv[side(d), i, 2].astype(F32)
        fin[i] = v.astype(BF16)
        for k in range(1, NZ):
            send(("fin", i, k), fin.at[i, wrow(zat(-k), 0, 64)], finr.at[k, i], zdev(-k))
        finr[0, i] = fin[i, own, :]

    def eg_own():
        return pltpu.make_async_copy(egs, eg_ref.at[strip(t)], lsem.at[11])

    def hid_flush():
        return pltpu.make_async_copy(hid_ref, hid_out, lsem.at[12])

    def dx_reduce():
        v = dxs[lax.div(t, 2)].astype(F32)
        got(("dx", 2), dxr.at[pl.ds(1, 3)])
        for k in (2, 6, 4):
            v = v + dxr[k // 2].astype(F32)
        for yp in range(NY // 2):
            for zp in range(2):
                a = v[:, 2 * yp * 256 + zp * LANE : 2 * yp * 256 + (zp + 1) * LANE]
                b = v[:, (2 * yp + 1) * 256 + zp * LANE : (2 * yp + 1) * 256 + (zp + 1) * LANE]
                low = low_lanes(a.shape)
                at0 = 2 * zp * 512 + yp * LANE
                egs[:, at0 : at0 + LANE] = jnp.where(low, a, swap_halves(b)).astype(BF16)
                egs[:, at0 + 512 : at0 + 512 + LANE] = jnp.where(low, swap_halves(a), b).astype(BF16)
        for k in (2, 6, 4):
            send(("eg", k), egs, eg_ref.at[strip(t)], tdev(k))
        send(("ec", 0), egs, eg_ref.at[strip(t)], pair)
        eg_own().start()

    def eg_cross():
        got(("eg", 2), dxr.at[pl.ds(1, 3)])
        for k in (2, 6, 4):
            here = eg_ref.at[strip(lax.rem(t + NT - k, NT))]
            send(("ec", k), here, here, pair)

    def eg_last():
        got(("ec", 0), dxc)

    def taps_finish():
        v = tys[...]
        got(("ty", 1), tyr.at[pl.ds(1, 7)])
        for k in range(1, NY):
            v = v + tyr[k]
        tfr[0] = v
        for k in range(1, NZ):
            send(("tf", k), tfr.at[0], tfr.at[k], zdev(-k))

    def late_pair(n, gpos, upos):
        _, gm, _ = mixed(prel, tile_cols(gpos))
        _, um, _ = mixed(prel, tile_cols(upos))
        act, _ = gelu_parts(gm)
        hid_ref[tile_cols(n), :] = (act * um).T.astype(BF16)

    def late_a(n, carry):
        late_pair(n, 2 * n, 2 * n + 1)
        return carry

    def late_b(m, carry):
        late_pair(m + 3, 2 * m + 7, 2 * m + 8)
        return carry

    def late_c():
        late_pair(2, 4, 5)
        _, mm, _ = mixed(prel, last)
        act, _ = gelu_parts(mm)
        hid_ref[640:HALF, :] = (act * swap_halves(mm)).T[0:64].astype(BF16)

    b1_take(1)
    a1_near("a")
    a2_own("a", 1)
    a2_own("a", 2)
    a2_take("a", 1, (0,))
    a1_far("a")
    a2_own("a", 3)
    b2_take(0)
    x_send(1)
    a2_take("a", 1, (1,))
    b1_take(2)
    x_send(2)
    a2_take("a", 1, (2,))
    a2_take("a", 1, (3,))
    b2_take(1)
    x_send(3)
    pulls[3].wait()
    order_rows(late_ref, xl)
    b1_take(3)
    a2_take("a", 2, (0, 1))
    project_a(0)
    a2_take("a", 2, (2, 3))
    b2_take(2)
    b1_take(4)
    x_take(1)
    a1_near("c")
    a1_far("c")
    a2_take("a", 3, (0,))
    a2_own("c", 0)
    project_a(1)
    a2_take("a", 3, (1,))
    a2_own("c", 1)
    a2_take("a", 3, (2,))
    a2_own("c", 2)
    a2_take("a", 3, (3,))
    a2_own("c", 3)
    x_take(2)
    project_a(2)
    a2_take("c", 1, (0,))
    a2_take("c", 1, (1,))
    x_take(3)
    a2_take("c", 1, (2,))
    project_a(3)
    b2_take(3)
    a2_take("c", 1, (3,))
    a2_take("a", 4, range(NZ))
    x_mid(1)
    b2_take(4)
    a2_take("c", 2, (0,))
    project_a(4)
    x_mid(2)
    a2_take("c", 2, (1,))
    pulls[4].wait()
    turn_cot()
    join_taps()
    lax.fori_loop(0, 2, early_a, 0)
    dp_send(0)
    a2_take("c", 2, (2,))
    b2f_take(0)
    project_b(0)
    x_far(1)
    a2_take("c", 2, (3,))
    b2f_take(1)
    project_b(1)
    x_mid(3)
    b2f_take(2)
    project_b(2)
    a2_take("c", 3, (0,))
    x_far(2)
    b2f_take(3)
    project_b(3)
    a2_take("c", 3, (1,))
    b2f_take(4)
    project_b(4)
    a2_take("c", 3, (2, 3))
    lax.fori_loop(0, 2, early_b, 0)
    dp_send(1)
    x_far(3)
    project_c(0)
    project_c(1)
    project_c(2)
    project_c(3)
    x_last()
    rs(0, 0)
    a2_take("c", 4, range(NZ))
    project_c(4)
    early_c()
    dp_send(2)
    lax.fori_loop(0, 4, dx, 0)
    rs(0, 1)
    lax.fori_loop(4, NY, dx, 0)
    dx_send()
    rs(1, 0)
    dx_pair()
    taps_first()
    rs(2, 0)
    rs(0, 2)
    rs(1, 1)
    late_project(wa, 0, 0, 256)
    late_project(wa, 0, 256, 256)
    late_project(wc, CA, 0, 256)
    late_project(wc, CA, 256, 128)
    rs(2, 1)
    dx_reduce()
    rs(0, 3)
    rs(1, 2)
    late_project(wb, AC, 0, 256)
    rs(2, 2)
    rs(1, 3)
    taps_finish()
    late_project(wb, AC, 256, 256)
    eg_cross()
    rs(2, 3)
    lax.fori_loop(0, 2, late_a, 0)
    lax.fori_loop(0, 2, late_b, 0)
    late_c()
    hid_flush().start()

    def spread(pos, v, prev, nxt):
        (gs, us), (gn, un) = prev, nxt
        if pos == 6:
            gn[:, 640:HALF] = gs[:, 640:HALF] + v[:, 0:64]
            un[:, 640:HALF] = us[:, 640:HALF] + swap_halves(v)[:, 0:64]
            return
        side_, n = (0, GPOS.index(pos)) if pos in GPOS else (1, UPOS.index(pos))
        cols = slice(n * LANE, (n + 1) * LANE)
        nxt[side_][:, cols] = prev[side_][:, cols] + v

    def tile_out(pos, v):
        spread(pos, v, (gsum_ref, usum_ref), (gnext_ref, unext_ref))

    def taps_out(pos, v):
        if pos == 6:
            gtnext_ref[:, 640:HALF] = gtsum_ref[:, 640:HALF] + v[0:3, 0:64]
            utnext_ref[:, 640:HALF] = utsum_ref[:, 640:HALF] + swap_halves(v)[0:3, 0:64]
            return
        spread(pos, v[0:3], (gtsum_ref, utsum_ref), (gtnext_ref, utnext_ref))

    def tf_take():
        got(("tf", 1), tfr.at[pl.ds(1, 3)])

    def fin_take(i):
        got(("fin", i, 1), finr.at[pl.ds(1, 3), i])

    def write_out(i):
        tiles = ((0, 1, 2, 3), (7, 8, 9, 10), (4, 5, 6))[i]
        for q, n in enumerate(tiles):
            k = lax.rem(q + NZ - z, NZ)
            tile_out(n, finr[k, i].astype(F32))
            taps_out(n, tfr[k, i])

    def sends_done():
        eg_own().wait()
        hid_flush().wait()
        gone("a1a", wa.at[0, pl.ds(0, 192)])
        gone("a1c", wc.at[0, pl.ds(0, 192)])
        gone("a2a", wa.at[pl.ds(0, 7)])
        gone("a2c", wc.at[pl.ds(0, 7)])
        gone("b1", wb.at[pl.ds(0, 7), pl.ds(0, 64)])
        gone("b2", wb.at[pl.ds(0, 4)])
        gone("b2f", wb.at[pl.ds(0, 2)])
        gone("x", xt.at[pl.ds(0, 6)])
        gone("rs", xt.at[pl.ds(0, 5), pl.ds(0, 3)])
        gone("fin", finr.at[pl.ds(0, 3)])
        gone("t", tyr.at[pl.ds(0, 6)])
        gone("ty", tyr.at[pl.ds(0, 7)])
        gone("d", xt.at[pl.ds(0, 7), pl.ds(0, 2)])

    pulls[5].wait()
    pulls[6].wait()
    tf_take()
    fin_take(0)
    write_out(0)
    fin_take(1)
    write_out(1)
    eg_last()
    fin_take(2)
    write_out(2)
    sends_done()


def flush(*refs):
    sem = refs[12]
    copies = [pltpu.make_async_copy(refs[n], refs[6 + n], sem.at[n]) for n in (1, 0, 2, 3, 4, 5)]
    for c in copies:
        c.start()
    for c in copies:
        c.wait()


def per_device(
    late_rows,
    early_rows,
    hidden_cot,
    gate_weight,
    up_weight,
    gate_taps,
    up_taps,
    gate_grad_sum,
    up_grad_sum,
    gate_taps_sum,
    up_taps_sum,
):
    vmem = pl.BlockSpec(memory_space=pltpu.VMEM)
    shapes = (
        ((HALF, ROWS), BF16),
        ((ROWS, 2048), BF16),
        ((64, HALF), F32),
        ((64, HALF), F32),
        ((3, HALF), F32),
        ((3, HALF), F32),
    )
    n_sem = 91
    hbm = pl.BlockSpec(memory_space=pltpu.HBM)
    hid, *rest = pl.pallas_call(
        kernel,
        out_shape=[pltpu.VMEM(s, d) for s, d in shapes],
        in_specs=[hbm] * 11,
        out_specs=[pl.BlockSpec(memory_space=pl.ANY)] * 2 + [vmem] * 4,
        scratch_shapes=[
            pltpu.VMEM((HALF, ROWS), BF16),
            pltpu.VMEM((ROWS, 2048), BF16),
            pltpu.VMEM((ROWS, 2048), BF16),
            pltpu.VMEM((HALF, ROWS), BF16),
            pltpu.VMEM((64, HALF), BF16),
            pltpu.VMEM((64, HALF), BF16),
            pltpu.VMEM((64, HALF), F32),
            pltpu.VMEM((64, HALF), F32),
            pltpu.VMEM((3, HALF), BF16),
            pltpu.VMEM((3, HALF), BF16),
            pltpu.VMEM((3, HALF), F32),
            pltpu.VMEM((3, HALF), F32),
            pltpu.VMEM((64, LANE), F32),
            pltpu.VMEM((8, WIDE), F32),
            pltpu.VMEM((NY, 256, CA), BF16),
            pltpu.VMEM((NY, 256, CC), BF16),
            pltpu.VMEM((NY, 256, CB), BF16),
            pltpu.VMEM((NY, ROWS, 256), BF16),
            pltpu.VMEM((NY, ROWS, 256), BF16),
            pltpu.VMEM((NY, NZ, 256, ROWS), BF16),
            pltpu.VMEM((ROWS, WIDE), F32),
            pltpu.VMEM((ROWS, WIDE), F32),
            pltpu.VMEM((ROWS, 768), BF16),
            pltpu.VMEM((ROWS, WIDE), BF16),
            pltpu.VMEM((3, NZ, ROWS, LANE), BF16),
            pltpu.VMEM((3, NZ, ROWS, LANE), BF16),
            pltpu.VMEM((2, 3, 4, 256, LANE), BF16),
            pltpu.VMEM((2, 3, 4, 256, LANE), BF16),
            pltpu.VMEM((3, 256, LANE), BF16),
            pltpu.VMEM((NZ, 3, 64, LANE), BF16),
            pltpu.VMEM((ROWS, 2048), BF16),
            pltpu.VMEM((4, 32, 2048), BF16),
            pltpu.VMEM((4, 32, 2048), BF16),
            pltpu.VMEM((4, 32, 2048), BF16),
            pltpu.VMEM((32, 2048), BF16),
            pltpu.VMEM((NZ, 3, 8, LANE), F32),
            pltpu.VMEM((NZ, 3, 8, LANE), F32),
            pltpu.VMEM((3, 8, LANE), F32),
            pltpu.VMEM((NY, 3, 8, LANE), F32),
            pltpu.VMEM((NZ, 3, 8, LANE), F32),
            pltpu.SemaphoreType.DMA((13,)),
            pltpu.SemaphoreType.DMA((13,)),
            pltpu.SemaphoreType.DMA((n_sem,)),
        ],
        compiler_params=pltpu.CompilerParams(
            collective_id=0, has_side_effects=True, vmem_limit_bytes=57000 * 1024
        ),
    )(
        late_rows,
        early_rows,
        hidden_cot.T,
        gate_weight,
        up_weight,
        gate_grad_sum,
        up_grad_sum,
        gate_taps,
        up_taps,
        gate_taps_sum,
        up_taps_sum,
    )
    hid, *rest = pl.pallas_call(
        flush,
        out_shape=[jax.ShapeDtypeStruct(s, d) for s, d in shapes],
        in_specs=[vmem] * 6,
        out_specs=[hbm] * 6,
        scratch_shapes=[pltpu.SemaphoreType.DMA((6,))],
        compiler_params=pltpu.CompilerParams(vmem_limit_bytes=8 * 1024 * 1024),
    )(hid, *rest)
    return (hid.T, *rest)


def solution(mesh):
    split = Mesh(
        mesh.devices.reshape(mesh.shape["rep"], NZ, NY, mesh.shape["tp"]),
        ("rep", "fs_0", "fs_1", "tp"),
    )
    placed = (
        P(REP_FS, None),
        P(REP_FS, None),
        P(REP_FS, "tp"),
        P(FS, "tp"),
        P(FS, "tp"),
        P(None, "tp"),
        P(None, "tp"),
        P(REP_FS, "tp"),
        P(REP_FS, "tp"),
        P("rep", "tp"),
        P("rep", "tp"),
    )
    return jax.shard_map(
        per_device,
        mesh=split,
        in_specs=placed,
        out_specs=(
            P(REP_FS, "tp"),
            P(REP_FS, None),
            P(REP_FS, "tp"),
            P(REP_FS, "tp"),
            P("rep", "tp"),
            P("rep", "tp"),
        ),
        check_vma=False,
    )
```
